32 devices in a mesh: ep: 8 (over z, x), tp: 4 (over y, core).
Axes of the slice: x: 2, y: 2, z: 4, core: 2. Of those that a mesh axis runs over, the one named last changes fastest.
Arguments:
- queries: bfloat16 [2048, 1024], P('ep', 'tp'), may hold values from -256 to 256
- key_rows: bfloat16 [2048, 1024], P('ep', 'tp'), may hold values from -8 to 8
- value_rows: bfloat16 [2048, 1024], P('ep', 'tp'), may hold values from -6 to 6
- head_lambda: float32 [8], P('tp'), may hold values from 0.3 to 0.8
- sub_gain: float32 [128], replicated, may hold values from 0.1 to 1.9
- out_weight: bfloat16 [1024, 2048], P('tp'), may hold values from -0.1875 to 0.1875
- expert_input: bfloat16 [1536, 2048], P('ep'), may hold values from -6 to 6
- norm_gain: float32 [2048], replicated, may hold values from 0.1 to 1.9
- route_ids: int32 [1536, 2], P('ep'), may hold values from 0 to 7, all different within a row; in each aligned block of 192 rows (0 to 191, 192 to 383, ...) at most 80 rows name the same one
- route_weight: float32 [1536, 2], P('ep'), may hold values from 0.25 to 1
- gate_weight: bfloat16 [8, 2048, 3584], P('ep', None, 'tp'), may hold values from -0.125 to 0.125
- up_weight: bfloat16 [8, 2048, 3584], P('ep', None, 'tp'), may hold values from -0.125 to 0.125
- down_weight: bfloat16 [8, 3584, 2048], P('ep', 'tp'), may hold values from -0.09375 to 0.09375
Outputs:
- mixer_out: bfloat16 [2048, 2048], P(('ep', 'tp'))
- expert_out: bfloat16 [1536, 2048], P('ep', 'tp')
The draws below stay inside these ranges and needn't reach their ends.
Inputs may be any that keep to these rules, and one draw needn't show every extreme that they name: `route_ids`: each row names 2 different experts. In each aligned block of 192 rows no expert is named by more than 80 rows, a bound that some block reaches.
All inputs are finite; a program needn't handle non-finite values.
Results may differ from the reference program's by a relative error of at most 0.014.
Values may be sent and summed in bfloat16 or wider, within the bound.
A program may use at most 256 MiB of HBM per device.

```python
import math
import jax
import jax.numpy as jnp
import numpy as np
from jax import lax

D = 2048
HEADS = 8
HEAD_DIM = 64
VALUE_DIM = 128
FF = 3584
TOP = 2
TOK_B_DEV = 192
EXPERTS = 8
CAP = 80
TOKENS_A = 2048
TOKENS_B = 1536
N_EP = 8
N_TP = 4


def query_key_pair(key):
    base = jax.random.fold_in(key, 11)
    key_draw, query_draw = jax.random.split(base, 2)
    shape = (TOKENS_A, HEADS, 2, HEAD_DIM)
    key_vals = 1.3 * jax.random.truncated_normal(key_draw, -6.0, 6.0, shape, jnp.float32)
    query_vals = 1.3 * jax.random.truncated_normal(query_draw, -6.0, 6.0, shape, jnp.float32)
    return (query_vals.reshape(TOKENS_A, HEADS * 2 * HEAD_DIM), key_vals.reshape(TOKENS_A, HEADS * 2 * HEAD_DIM))


def draw_queries(key, part):
    return query_key_pair(key)[0].astype(jnp.bfloat16)


def draw_key_rows(key, part):
    return query_key_pair(key)[1].astype(jnp.bfloat16)


def block_scale(stream_key, dims, cuts, smallest, largest):
    loudness, own = 1.0, jax.random.fold_in(stream_key, 6)
    for position, parts in cuts:
        draws = jnp.exp(jax.random.uniform(jax.random.fold_in(own, position), (parts,), jnp.float32, smallest / len(cuts), largest / len(cuts)))
        loudness = loudness * jnp.repeat(draws, dims[position] // parts).reshape([-1 if axis == position else 1 for axis in range(len(dims))])
    return loudness


def shared_out(stream_key, own, number, rows, count, top, limit, skew):
    order = jax.random.permutation(stream_key, count)
    heavy_load, usual = portions_of(count, rows * top, limit, skew, True), portions_of(count, rows * top, limit, skew, False)
    places = jnp.arange(count)

    def named(lengths, offset_by):
        used = int((lengths > 0).sum())
        fixed = max(1, used // 4)
        passed = fixed + (places - fixed + offset_by * (used - fixed)) % max(1, count - fixed)
        return jnp.zeros((count,), jnp.int32).at[order[jnp.where(places < fixed, places, passed)]].set(jnp.asarray(lengths, jnp.int32))

    lengths = jnp.where(number % 4 == 0, named(heavy_load, number // 4), named(usual, number - number // 4 - 1))
    mixed = jax.random.permutation(jax.random.fold_in(own, 3), count)
    source_of, receiver = mixed[0:count // 2 * 2:2], mixed[1:count // 2 * 2:2]
    slack = jnp.minimum(lengths[source_of] - 1, limit - lengths[receiver]) // 2
    slack = jnp.where((source_of == order[0]) | (receiver == order[0]) | (lengths[receiver] == 0), 0, jnp.maximum(slack, 0))
    passed = jax.random.randint(jax.random.fold_in(own, 4), (count // 2,), 0, 1 << 20) % (slack + 1)
    lengths = lengths.at[source_of].add(-passed).at[receiver].add(passed)
    items = jnp.searchsorted(jnp.cumsum(lengths), jnp.arange(rows * top), side="right").astype(jnp.int32)
    grid = items.reshape(top, rows).T
    grid = grid[jax.random.permutation(jax.random.fold_in(own, 1), rows)]
    offset_by = jax.random.randint(jax.random.fold_in(own, 2), (rows, 1), 0, top)
    return jnp.take_along_axis(grid, (jnp.arange(top)[None, :] + offset_by) % top, axis=1)


def portions_of(amount, total, limit, skew, full):
    loads = [(1 << 20) // math.isqrt(standing ** skew) + 1 for standing in range(1, amount + 1)]
    largest = limit if full else min(limit, max(-(-total // amount), total * loads[0] // sum(loads)))
    least = 1 if total - largest >= amount - 1 else 0
    holding, rest = [largest] + [least] * (amount - 1), total - largest - least * (amount - 1)
    while rest > 0:
        free = [i for i in range(1, amount) if holding[i] < largest] or [i for i in range(1, amount) if holding[i] < limit]
        whole, budget = sum([loads[i] for i in free]), rest
        for i in free:
            addition = min(limit - holding[i], max(1, budget * loads[i] // whole), rest)
            holding[i] = holding[i] + addition
            rest = rest - addition
    return np.array(holding)


def noise(key, shape, spread, reach, shards=(), kind=jnp.bfloat16):
    level = block_scale(key, shape, shards, -0.22, 0.18) if shards else 1.0
    entries = jax.random.normal(key, shape, jnp.float32) * spread * level
    return jnp.minimum(jnp.maximum(entries, -reach), reach).astype(kind)


def setup_inputs(seed: int = 0) -> dict:
    arg_keys = jax.random.split(jax.random.key(seed), 14)
    queries = draw_queries(jax.random.fold_in(arg_keys[13], 71), 0)
    key_rows = draw_key_rows(jax.random.fold_in(arg_keys[13], 71), 0)
    value_rows = noise(arg_keys[2], (TOKENS_A, HEADS * VALUE_DIM), 1.0, 6.0, ((0, 8), (1, 4)))
    head_lambda = jnp.clip(0.3 + 0.5 * jax.random.uniform(arg_keys[3], (HEADS,), jnp.float32) ** block_scale(arg_keys[3], (HEADS,), ((0, 4),), -0.2, 0.2), 0.3, 0.8)
    sub_gain = jnp.clip(1.0 + 0.18 * jax.random.normal(arg_keys[4], (VALUE_DIM,), jnp.float32), 0.1, 1.9)
    out_weight = noise(arg_keys[5], (HEADS * VALUE_DIM, D), (HEADS * VALUE_DIM) ** -0.5, 0.1875, ((0, 4),))
    expert_input = noise(arg_keys[6], (TOKENS_B, D), 1.0, 6.0, ((0, 8),))
    norm_gain = jnp.clip(1.0 + 0.18 * jax.random.normal(arg_keys[7], (D,), jnp.float32), 0.1, 1.9)
    route_ids_keys = jax.random.split(jax.random.fold_in(arg_keys[8], 1), TOKENS_B // TOK_B_DEV)
    route_ids_turns = jax.random.permutation(jax.random.fold_in(arg_keys[8], 3), TOKENS_B // TOK_B_DEV)
    route_ids = jax.vmap(lambda own, number: shared_out(jax.random.fold_in(arg_keys[8], 2), own, number, TOK_B_DEV, EXPERTS, TOP, CAP, 1))(route_ids_keys, route_ids_turns).reshape((TOKENS_B, TOP))
    route_weight = jnp.clip(0.25 + 0.75 * jax.random.uniform(arg_keys[9], (TOKENS_B, TOP), jnp.float32) ** block_scale(arg_keys[9], (TOKENS_B, TOP), ((0, 8),), -0.2, 0.2), 0.25, 1.0)
    gate_weight = noise(arg_keys[10], (EXPERTS, D, FF), D ** -0.5, 0.125, ((0, 8), (2, 4)))
    up_weight = noise(arg_keys[11], (EXPERTS, D, FF), D ** -0.5, 0.125, ((0, 8), (2, 4)))
    down_weight = noise(arg_keys[12], (EXPERTS, FF, D), FF ** -0.5, 0.09375, ((0, 8), (1, 4)))
    return {"queries": queries, "key_rows": key_rows, "value_rows": value_rows, "head_lambda": head_lambda, "sub_gain": sub_gain, "out_weight": out_weight, "expert_input": expert_input, "norm_gain": norm_gain, "route_ids": route_ids, "route_weight": route_weight, "gate_weight": gate_weight, "up_weight": up_weight, "down_weight": down_weight}


EPS = 1e-06

def round_keep(values):
    return lax.optimization_barrier(values.astype(jnp.bfloat16)).astype(jnp.float32)

def head_output(query_head, key_head, value_head, lam_value, sub_gain):
    block_rows = math.gcd(TOKENS_A, 512)
    scaling = HEAD_DIM ** (-0.5)
    key_pos = jnp.arange(TOKENS_A, dtype=jnp.int32)
    key_wide = key_head.astype(jnp.float32)
    value_wide = value_head.astype(jnp.float32)

    def one_block(block_index):
        first_row = (block_index * block_rows).astype(jnp.int32)
        query_block = lax.dynamic_slice_in_dim(query_head, first_row, block_rows, 0).astype(jnp.float32)
        scores = jnp.einsum('qmd,kmd->mqk', query_block, key_wide) * scaling
        query_pos = first_row + jnp.arange(block_rows, dtype=jnp.int32)
        allowed = query_pos[:, None] >= key_pos[None, :]
        scores = jnp.where(allowed, scores, -jnp.inf)
        row_max = lax.optimization_barrier(jnp.max(scores, axis=-1, keepdims=True))
        weights = jnp.where(allowed, jnp.exp(scores - row_max), 0.0)
        row_total = lax.optimization_barrier(jnp.sum(weights, axis=-1))
        numerator = jnp.einsum('mqk,kd->mqd', round_keep(weights), value_wide)
        per_map = numerator / row_total[..., None]
        contrast = per_map[0] - lam_value * per_map[1]
        normed = contrast * lax.rsqrt(lax.optimization_barrier(jnp.mean(contrast * contrast, axis=-1, keepdims=True)) + EPS) * sub_gain
        return normed.astype(jnp.bfloat16)
    blocks = lax.map(one_block, jnp.arange(TOKENS_A // block_rows, dtype=jnp.int32))
    return blocks.reshape(TOKENS_A, VALUE_DIM)

def reference(queries, key_rows, value_rows, head_lambda, sub_gain, out_weight, expert_input, norm_gain, route_ids, route_weight, gate_weight, up_weight, down_weight):
    query_heads = jnp.moveaxis(queries.reshape(TOKENS_A, HEADS, 2, HEAD_DIM), 1, 0)
    key_heads = jnp.moveaxis(key_rows.reshape(TOKENS_A, HEADS, 2, HEAD_DIM), 1, 0)
    value_heads = jnp.moveaxis(value_rows.reshape(TOKENS_A, HEADS, VALUE_DIM), 1, 0)

    def per_head(operands):
        return head_output(operands[0], operands[1], operands[2], operands[3], sub_gain)
    attended = lax.map(per_head, (query_heads, key_heads, value_heads, head_lambda))
    attended = jnp.moveaxis(attended, 0, 1).reshape(TOKENS_A, HEADS * VALUE_DIM)
    group_cols = HEADS // N_TP * VALUE_DIM
    mixed_sum = jnp.zeros((TOKENS_A, D), jnp.float32)
    for group_index in range(N_TP):
        lower = group_index * group_cols
        share = jnp.dot(attended[:, lower:lower + group_cols], out_weight[lower:lower + group_cols], preferred_element_type=jnp.float32)
        mixed_sum = mixed_sum + round_keep(share)
    mixer_out = mixed_sum.astype(jnp.bfloat16)
    wide_rows = expert_input.astype(jnp.float32)
    normed_input = (wide_rows * lax.rsqrt(lax.optimization_barrier(jnp.mean(wide_rows * wide_rows, axis=-1, keepdims=True)) + EPS) * norm_gain).astype(jnp.bfloat16)
    flat_ids = route_ids.reshape(N_EP, TOK_B_DEV * TOP)
    onehot = (flat_ids[..., None] == jnp.arange(EXPERTS, dtype=jnp.int32)).astype(jnp.int32)
    rank_before = jnp.cumsum(onehot, axis=1) - onehot
    slot_index = lax.optimization_barrier(jnp.sum(rank_before * onehot, axis=-1))
    source = jnp.arange(N_EP, dtype=jnp.int32)[:, None]
    buffer_pos = ((flat_ids * N_EP + source) * CAP + slot_index).astype(jnp.int32)
    token_index = (source * TOK_B_DEV + jnp.arange(TOK_B_DEV * TOP, dtype=jnp.int32)[None, :] // TOP).astype(jnp.int32)
    row_table = jnp.full((EXPERTS * N_EP * CAP,), TOKENS_B, jnp.int32)
    row_table = row_table.at[buffer_pos.reshape(-1)].set(token_index.reshape(-1))
    padded = jnp.concatenate([normed_input, jnp.zeros((1, D), jnp.bfloat16)], axis=0)
    unit_share = FF // N_TP

    def one_expert(operands):
        gathered = padded[operands[0]]
        gate_act = jnp.dot(gathered, operands[1], preferred_element_type=jnp.float32)
        up_act = jnp.dot(gathered, operands[2], preferred_element_type=jnp.float32)
        hidden = (jax.nn.silu(gate_act) * up_act).astype(jnp.bfloat16)
        result_sum = jnp.zeros((N_EP * CAP, D), jnp.float32)
        for group_index in range(N_TP):
            lower = group_index * unit_share
            share = jnp.dot(hidden[:, lower:lower + unit_share], operands[3][lower:lower + unit_share], preferred_element_type=jnp.float32)
            result_sum = result_sum + round_keep(share)
        return result_sum.astype(jnp.bfloat16)
    results = lax.map(one_expert, (row_table.reshape(EXPERTS, N_EP * CAP), gate_weight, up_weight, down_weight))
    picked = results.reshape(EXPERTS * N_EP * CAP, D)[buffer_pos.reshape(-1)]
    picked = picked.reshape(TOKENS_B, TOP, D).astype(jnp.float32)
    expert_out = lax.optimization_barrier(jnp.sum(picked * route_weight[..., None], axis=1)).astype(jnp.bfloat16)
    return (mixer_out, expert_out)
```

```python
import functools

import jax
import jax.numpy as jnp
from jax import lax
from jax.experimental import pallas as pl
from jax.experimental.pallas import tpu as pltpu
from jax.sharding import PartitionSpec as P

EPS = 1e-06
MESH = pl.DeviceIdType.MESH
F32 = jnp.float32
BF16 = jnp.bfloat16


def flip(index, bits):
    low = 1
    while low <= bits:
        if bits & low:
            index = index + low - 2 * low * ((index // low) % 2)
        low *= 2
    return index


def dot(a, b, dims=((1,), (0,)), precision=None):
    return lax.dot_general(a, b, (dims, ((), ())), precision=precision, preferred_element_type=F32)


def kernel(
    n_ep, cap, lam, q, k, v, gain, x, norm_gain, ids, route_w, wo_hbm, wg_hbm, wu_hbm, wd_hbm,
    mixer, expert,
    wo, wg, wu, wd, arr, hidden, part, sib, ysend, yrecv, res, ret, kbuf, vbuf,
    outb, nrm, info, nrm_in, info_in, spread, qx, qs, high, low, acc, top, mix, att, hp, hsib, hysend, hyrecv,
    w_sem, d_send, d_recv, f_send, f_recv, r_send, r_recv, s_send, s_recv, y_send, y_recv,
    g_send, g_recv, x_send, x_recv, kv_send, kv_recv, k2_send, h_send, h_recv,
):
    me = lax.axis_index("ep")
    tp = lax.axis_index("tp")
    half, quarter = n_ep // 2, n_ep // 4
    upper = me // half
    near = (upper * half, half)
    inner = (half - upper * quarter, quarter)
    outer = ((1 - upper) * (half + quarter), quarter)
    mate = flip(me, half + quarter)
    first = upper * half
    tokens, width = x.shape
    cols = width // 4
    units = wg.shape[1]
    sib_tp, y_tp = flip(tp, 1), flip(tp, 2)

    def remote(src, dst, ssem, rsem, where):
        return pltpu.make_async_remote_copy(
            src_ref=src, dst_ref=dst, send_sem=ssem, recv_sem=rsem,
            device_id=where, device_id_type=MESH,
        )

    weights = [
        pltpu.make_async_copy(a, b, w_sem.at[i])
        for i, (a, b) in enumerate(((wg_hbm, wg), (wu_hbm, wu), (wd_hbm, wd), (wo_hbm, wo)))
    ]
    for copy in weights:
        copy.start()

    barrier = pltpu.get_barrier_semaphore()
    for d in range(1, n_ep):
        pl.semaphore_signal(barrier, inc=1, device_id=(flip(me, d), tp), device_id_type=MESH)
    for d in range(1, 4):
        pl.semaphore_signal(barrier, inc=1, device_id=(me, flip(tp, d)), device_id_type=MESH)

    slots = n_ep * cap
    id0, id1 = ids[0:1, :], ids[1:2, :]
    index = lax.broadcasted_iota(jnp.int32, (max(n_ep, 8), tokens), 0)
    hot0, hot1 = (index == id0).astype(F32), (index == id1).astype(F32)
    earlier = (
        lax.broadcasted_iota(jnp.int32, (tokens, tokens), 0)
        < lax.broadcasted_iota(jnp.int32, (tokens, tokens), 1)
    ).astype(F32).astype(BF16)
    rank = dot((hot0 + hot1).astype(BF16), earlier)
    row0 = id0 * cap + (jnp.sum(rank * hot0, axis=0, keepdims=True) + 0.5).astype(jnp.int32)
    row1 = id1 * cap + (jnp.sum(rank * hot1, axis=0, keepdims=True) + 0.5).astype(jnp.int32)
    slot = lax.broadcasted_iota(jnp.int32, (slots, tokens), 0)
    here = lax.broadcasted_iota(jnp.int32, (half * cap, tokens), 0) + first * cap
    dispatch = ((here == row0) | (here == row1)).astype(F32).astype(BF16)
    wide = x[...].astype(F32)
    inv = lax.rsqrt(jnp.mean(wide * wide, axis=-1, keepdims=True) + EPS)
    mine = pl.ds(pl.multiple_of(tp * cols, cols), cols)
    normed = (x[:, mine].astype(F32) * inv * norm_gain[:, mine]).astype(BF16)
    nrm[...] = normed
    line = lax.broadcasted_iota(jnp.int32, (8, tokens), 0)
    info[...] = jnp.where(line == 0, row0, jnp.where(line == 1, row1, 0)).astype(F32)
    outb[...] = dot(dispatch, normed).astype(BF16).reshape(half, cap, cols)
    pl.semaphore_wait(barrier, n_ep - 1 + 3)

    def dispatch_to(at):
        return remote(outb.at[at - first], arr.at[tp, me], d_send.at[at], d_recv.at[me], (at, tp))

    def spread_to(at):
        return remote(
            spread.at[at - first], arr.at[tp, mate], d_send.at[flip(at, half)], d_recv.at[mate], (at, tp)
        )

    def dispatch_from(at):
        return remote(outb.at[0], arr.at[tp, at], d_send.at[at], d_recv.at[at], (at, tp))

    def to_mate(i):
        src, dst = ((info, info_in), (nrm, nrm_in))[i]
        return remote(src, dst, g_send.at[i], g_recv.at[i], (mate, tp))

    def sources(group):
        base, size = group
        return [flip(base + me % size, i) for i in range(size)]

    def others(group):
        return sources(group)[1:] if group is near else sources(group)

    def send(ds):
        for d in ds:
            dispatch_to(flip(me, d)).start()

    def send_mate():
        to_mate(0).start()
        to_mate(1).start()

    at_middle = (me // quarter == 1) | (me // quarter == 2)

    def expand(condition):
        @pl.when(condition)
        def _():
            to_mate(0).wait_recv()
            to_mate(1).wait_recv()
            place = here.astype(F32)
            pick = ((place == info_in[0:1]) | (place == info_in[1:2])).astype(F32).astype(BF16)
            spread[...] = dot(pick, nrm_in[...]).astype(BF16).reshape(half, cap, cols)
            for at in others(near):
                spread_to(at).start()
            arr[tp, mate] = spread[me - first]

    def own_rows():
        local = lax.broadcasted_iota(jnp.int32, (cap, tokens), 0) + me * cap
        pick = ((local == row0) | (local == row1)).astype(F32).astype(BF16)
        for t in range(4):
            at = slice(t * cols, (t + 1) * cols)
            rows = (x[:, at].astype(F32) * inv * norm_gain[:, at]).astype(BF16)
            arr[t, me] = dot(pick, rows).astype(BF16)

    def weigh():
        comb = jnp.where(slot == row0, route_w[0:1, :], 0.0) + jnp.where(
            slot == row1, route_w[1:2, :], 0.0
        )
        big = comb.astype(BF16).astype(F32)
        high[...] = comb.T.astype(BF16)
        low[...] = (comb - big).T.astype(BF16)

    def to_sib(src):
        return remote(
            arr.at[tp, src], arr.at[tp, src], f_send.at[0, src], f_recv.at[0, src], (me, sib_tp)
        )

    def to_y(src):
        return remote(
            arr.at[tp, src], arr.at[tp, src], f_send.at[1, src], f_recv.at[1, src], (me, y_tp)
        )

    def y_to_sib(src):
        return remote(
            arr.at[y_tp, src], arr.at[y_tp, src], f_send.at[2, src], f_recv.at[2, src], (me, sib_tp)
        )

    def forward(src):
        @pl.when(src != mate)
        def _():
            dispatch_from(src).wait_recv()

        to_y(src).start()
        to_sib(src).start()

    def relay(src):
        to_y(src).wait_recv()
        y_to_sib(src).start()

    def arrived(src):
        to_sib(src).wait_recv()
        y_to_sib(src).wait_recv()

    def gate_up(group, lo, hi):
        base, rows = group[0], group[1] * cap
        got = [arr[t, pl.ds(base, group[1])].reshape(rows, cols) for t in range(4)]
        for lo in range(lo * 128, min(hi * 128, units), 256):
            n = min(256, units - lo)
            total = jnp.zeros((rows, 2 * n), F32)
            for t in range(4):
                at = slice(t * cols, (t + 1) * cols)
                w = jnp.concatenate([wg[at, lo:lo + n], wu[at, lo:lo + n]], axis=1)
                total += dot(got[t], w)
            g, u = total[:, :n], total[:, n:]
            hidden[:rows, lo:lo + n] = (g / (1.0 + jnp.exp(-g)) * u).astype(BF16)

    def down(group, r):
        base, rows = group[0], group[1] * cap
        at = pl.ds(pl.multiple_of(flip(tp, r) * cols, cols), cols)
        out = dot(hidden[:rows], wd[:, at])
        part[r, pl.ds(base, group[1])] = out.astype(BF16).reshape(group[1], cap, cols)

    pairs = {}

    def pair(group, number, y):
        at = pl.ds(*group)
        c = remote(
            part.at[2 * y + 1, at], sib.at[y, at], s_send.at[number, y], s_recv.at[number, y], (me, sib_tp)
        )
        c.start()
        pairs[number, y] = c

    def over_y(at):
        return remote(ysend.at[at], yrecv.at[at], y_send.at[at], y_recv.at[at], (me, y_tp))

    def y_sum(group, number):
        pairs[number, 1].wait_recv()
        at = pl.ds(*group)
        ysend[at] = (part[2, at].astype(F32) + sib[1, at].astype(F32)).astype(BF16)

    def y_go(srcs):
        for to in srcs:
            over_y(to).start()

    def return_to(at):
        return remote(res.at[at], ret.at[me], r_send.at[at], r_recv.at[me], (at, tp))

    def return_from(at):
        return remote(res.at[at], ret.at[at], r_send.at[at], r_recv.at[at], (at, tp))

    def give_back(to, own=False):
        over_y(to).wait_recv()
        out = (
            part[0, to].astype(F32) + sib[0, to].astype(F32) + yrecv[to].astype(F32)
        ).astype(BF16)
        if own:
            ret[to] = out
        else:
            res[to] = out
            return_to(to).start()

    across = flip(me, 1)
    level, side = me // 2, me % 2
    levels = n_ep // 2
    pinch = levels // 2 - 1

    q_rows = q.shape[0]
    heads = lam.shape[0]
    pair_width = q.shape[1] // heads
    head_width = pair_width // 2
    other = 1 - side
    my_head = pl.ds(pl.multiple_of(side * pair_width, pair_width), pair_width)
    its_head = pl.ds(pl.multiple_of(other * pair_width, pair_width), pair_width)

    def swap(i):
        src, dst = ((k, kbuf.at[level, side]), (v, vbuf.at[level, side]), (q, qx.at[side]))[i]
        return remote(src.at[:, its_head], dst, x_send.at[i], x_recv.at[i], (across, tp))

    def swap_start():
        for i in range(3):
            swap(i).start()
        kbuf[level, side] = k[:, my_head]
        vbuf[level, side] = v[:, my_head]
        qx[side] = q[:, my_head]

    def swap_wait():
        for i in range(3):
            swap(i).wait_recv()

    def kv_copy(b, lev):
        buf = kbuf if b < 2 else vbuf
        at = buf.at[lev, b % 2]
        return remote(at, at, kv_send.at[b, lev], kv_recv.at[b, lev], (lax.rem(me + 2, n_ep), tp))

    def kv_skip(b):
        buf = kbuf if b < 2 else vbuf
        at = buf.at[level, b % 2]
        return remote(at, at, k2_send.at[b], kv_recv.at[b, level], (lax.rem(me + 4, n_ep), tp))

    def kv_first():
        @pl.when(level == pinch - 1)
        def _():
            for b in range(4):
                kv_skip(b).start()

        @pl.when(level < levels - 1)
        def _():
            for b in range(4):
                kv_copy(b, level).start()

    def kv_hop(step):
        for b in range(4):
            kv_copy(b, level - step).wait_recv()
            kv_copy(b, level - step).start()

    def hop_lower():
        for step in range(1, pinch + 1):
            @pl.when((level >= step) & ((level < pinch) | ((level == pinch) & (step > 1))))
            def _():
                kv_hop(step)

    def hop_upper(lo, hi):
        for step in range(lo, hi):
            @pl.when((level > pinch) & (level < levels - 1) & (level >= step))
            def _():
                kv_hop(step)

    def kv_last(step):
        @pl.when(((level == levels - 1) & (level >= step)) | ((level == pinch) & (step == 1)))
        def _():
            for b in range(4):
                kv_copy(b, level - step).wait_recv()

    def kv_finish():
        def step(lev, carry):
            for b in range(4):
                kv_copy(b, lev).wait_send()
            return carry

        @pl.when((level < levels - 1) & (level != pinch))
        def _():
            lax.fori_loop(0, level + 1, step, 0)

        @pl.when(level == pinch)
        def _():
            lax.fori_loop(0, level - 1, step, 0)
            step(level, 0)

        @pl.when(level == pinch - 1)
        def _():
            for b in range(4):
                kv_skip(b).wait_send()

    both = 2 * q_rows
    head_lane = lax.broadcasted_iota(jnp.int32, (both, pair_width), 1)

    def with_ones(vb):
        return jnp.concatenate([vb, jnp.ones(vb.shape, BF16)], axis=1)

    def attend_own():
        qh = qx[...].reshape(both, pair_width).astype(F32) * (head_width ** -0.5)
        kb = kbuf[level].reshape(both, pair_width)
        vb = with_ones(vbuf[level].reshape(both, pair_width))
        for m in range(2):
            first = head_lane < head_width
            qs[m] = jnp.where(first if m == 0 else ~first, qh, 0.0).astype(BF16)
            s = dot(qs[m], kb, ((1,), (1,)))
            ok = lax.broadcasted_iota(jnp.int32, s.shape, 0) >= lax.broadcasted_iota(jnp.int32, s.shape, 1)
            s = jnp.where(ok, s, -1e30)
            t = jnp.max(s, axis=1, keepdims=True)
            w = jnp.exp(s - t)
            top[m] = t
            acc[m] = dot(w.astype(BF16), vb)

    def attend(lev):
        kb = kbuf[lev].reshape(both, pair_width)
        vb = with_ones(vbuf[lev].reshape(both, pair_width))
        for m in range(2):
            s = dot(qs[m], kb, ((1,), (1,)))
            old = top[m]
            t = jnp.maximum(old, jnp.max(s, axis=1, keepdims=True))
            w = jnp.exp(s - t)
            top[m] = t
            acc[m] = acc[m] * jnp.exp(old - t) + dot(w.astype(BF16), vb)

    def attend_at(step):
        @pl.when(level >= step)
        def _():
            attend(level - step)

    def att_swap():
        return remote(mix.at[other], att.at[side], x_send.at[3], x_recv.at[3], (across, tp))

    def normalise():
        a = acc[:, :, :pair_width] / acc[:, :, pair_width:]
        contrast = a[0] - lam[side] * a[1]
        norm = lax.rsqrt(jnp.mean(contrast * contrast, axis=-1, keepdims=True) + EPS)
        mix[...] = (contrast * norm * gain[...]).astype(BF16).reshape(2, q_rows, pair_width)
        att_swap().start()
        att[side] = mix[side]

    def h_pair(y):
        return remote(
            hp.at[flip(tp, 2 * y + 1)], hsib.at[y], h_send.at[y], h_recv.at[y], (me, sib_tp)
        )

    def h_over():
        return remote(hysend, hyrecv, h_send.at[2], h_recv.at[2], (me, y_tp))

    def project():
        att_swap().wait_recv()
        rows = jnp.concatenate([att[h] for h in range(heads)], axis=1)
        hp[...] = dot(rows, wo[...]).astype(BF16).reshape(4, q_rows // 4, width)
        h_pair(1).start()
        h_pair(0).start()

    def h_send_over():
        h_pair(1).wait_recv()
        hysend[...] = (hp[y_tp].astype(F32) + hsib[1].astype(F32)).astype(BF16)
        h_over().start()

    def drain():
        for src in others(near) + sources(inner) + sources(outer):
            to_sib(src).wait_send()
            to_y(src).wait_send()
            y_to_sib(src).wait_send()
            return_to(src).wait_send()
        for src in sources(near) + sources(inner) + sources(outer):
            over_y(src).wait_send()
        for at in others(near):
            dispatch_to(at).wait_send()
            spread_to(at).wait_send()
        for i in range(2):
            to_mate(i).wait_send()
        for c in pairs.values():
            c.wait_send()
        for y in range(2):
            h_pair(y).wait_send()
        for i in range(3):
            swap(i).wait_send()
        att_swap().wait_send()
        kv_finish()

    def mix_out():
        h_pair(0).wait_recv()
        h_over().wait()
        mixer[...] = (
            hp[tp].astype(F32) + hsib[0].astype(F32) + hyrecv[...].astype(F32)
        ).astype(BF16)

    def combine():
        for src in others(near) + sources(inner) + sources(outer):
            return_from(src).wait_recv()
        got = ret[...].reshape(slots, cols)
        expert[...] = (dot(high[...], got) + dot(low[...], got)).astype(BF16)

    send(range(1, half))
    send_mate()
    own_rows()
    weigh()
    forward(others(near)[0])
    swap_start()
    forward(others(near)[1])
    for at in others(near)[2:]: forward(at)
    expand(at_middle)
    relay(others(near)[0])
    swap_wait()
    expand(~at_middle)
    kv_first()
    for at in others(near)[1:]: relay(at)
    for at in sources(inner)[:1]: forward(at)
    for copy in weights[:2]: copy.wait()
    for at in sources(inner)[1:]: forward(at)
    for at in others(near): arrived(at)
    gate_up(near, 0, 4)
    for at in sources(outer)[:1]: forward(at)
    for at in sources(inner)[:1]: relay(at)
    gate_up(near, 4, 7)
    for at in sources(outer)[1:]: forward(at)
    for at in sources(inner)[1:]: relay(at)
    weights[2].wait()
    for r in (3, 1): down(near, r)
    pair(near, 0, 1)
    pair(near, 0, 0)
    for r in (2, 0): down(near, r)
    for at in sources(inner): arrived(at)
    gate_up(inner, 0, 7)
    for at in sources(outer)[:1]: relay(at)
    hop_lower()
    down(inner, 3)
    pair(inner, 1, 1)
    down(inner, 2)
    for at in sources(outer)[1:]: relay(at)
    hop_upper(1, 2)
    down(inner, 1)
    pair(inner, 1, 0)
    down(inner, 0)
    y_sum(inner, 1)
    y_go(sources(inner))
    for at in sources(outer): arrived(at)
    gate_up(outer, 0, 7)
    hop_upper(2, levels)
    down(outer, 3)
    pair(outer, 2, 1)
    down(outer, 2)
    down(outer, 1)
    pair(outer, 2, 0)
    down(outer, 0)
    y_sum(outer, 2)
    y_go(sources(outer))
    y_sum(near, 0)
    y_go(sources(near))
    attend_own()
    pairs[1, 0].wait_recv()
    for at in sources(inner): give_back(at)
    kv_last(1)
    attend_at(1)
    pairs[2, 0].wait_recv()
    for at in sources(outer): give_back(at)
    for step in range(2, levels): kv_last(step); attend_at(step)
    normalise()
    pairs[0, 0].wait_recv()
    for i, at in enumerate(sources(near)): give_back(at, i == 0)
    weights[3].wait()
    project()
    h_send_over()
    combine()
    drain()
    mix_out()


def settle(mixer_in, expert_in, mixer, expert, a, b, load, store):
    pairs = ((mixer_in, a, mixer), (expert_in, b, expert))
    loads = [pltpu.make_async_copy(x, y, load.at[i]) for i, (x, y, _) in enumerate(pairs)]
    stores = [pltpu.make_async_copy(y, z, store.at[i]) for i, (_, y, z) in enumerate(pairs)]
    for copy in loads:
        copy.start()
    for i in range(2):
        loads[i].wait()
        stores[i].start()
    for copy in stores:
        copy.wait()


def solution(mesh):
    n_ep = mesh.shape["ep"]

    def shards(
        queries, key_rows, value_rows, head_lambda, sub_gain, out_weight, expert_input, norm_gain,
        route_ids, route_weight, gate_weight, up_weight, down_weight,
    ):
        tokens, width = expert_input.shape
        cap = 5 * route_ids.shape[1] * tokens // (3 * n_ep)
        cap = -(-cap // 16) * 16
        cols = width // 4
        half = n_ep // 2
        units = gate_weight.shape[2]
        q_rows, kv_cols = queries.shape
        heads = head_lambda.shape[0]
        vm = pl.BlockSpec(memory_space=pltpu.VMEM)
        hbm = pl.BlockSpec(memory_space=pl.ANY)
        dma = pltpu.SemaphoreType.DMA
        outs = pl.pallas_call(
            functools.partial(kernel, n_ep, cap),
            name="both_halves",
            out_shape=(
                jax.ShapeDtypeStruct((q_rows // 4, width), BF16),
                jax.ShapeDtypeStruct((tokens, cols), BF16),
            ),
            in_specs=[pl.BlockSpec(memory_space=pltpu.SMEM)] + [vm] * 8 + [hbm] * 4,
            out_specs=(vm, vm),
            scratch_shapes=[
                pltpu.VMEM(out_weight.shape, BF16),
                pltpu.VMEM((width, units), BF16),
                pltpu.VMEM((width, units), BF16),
                pltpu.VMEM((units, width), BF16),
                pltpu.VMEM((4, n_ep, cap, cols), BF16),
                pltpu.VMEM((half * cap, units), BF16),
                pltpu.VMEM((4, n_ep, cap, cols), BF16),
                pltpu.VMEM((2, n_ep, cap, cols), BF16),
                pltpu.VMEM((n_ep, cap, cols), BF16),
                pltpu.VMEM((n_ep, cap, cols), BF16),
                pltpu.VMEM((n_ep, cap, cols), BF16),
                pltpu.VMEM((n_ep, cap, cols), BF16),
                pltpu.VMEM((half, 2, q_rows, kv_cols // heads), BF16),
                pltpu.VMEM((half, 2, q_rows, kv_cols // heads), BF16),
                pltpu.VMEM((half, cap, cols), BF16),
                pltpu.VMEM((tokens, cols), BF16),
                pltpu.VMEM((8, tokens), F32),
                pltpu.VMEM((tokens, cols), BF16),
                pltpu.VMEM((8, tokens), F32),
                pltpu.VMEM((half, cap, cols), BF16),
                pltpu.VMEM((2, q_rows, kv_cols // heads), BF16),
                pltpu.VMEM((2, 2 * q_rows, kv_cols // heads), BF16),
                pltpu.VMEM((tokens, n_ep * cap), BF16),
                pltpu.VMEM((tokens, n_ep * cap), BF16),
                pltpu.VMEM((2, 2 * q_rows, 2 * kv_cols // heads), F32),
                pltpu.VMEM((2, 2 * q_rows, 1), F32),
                pltpu.VMEM((2, q_rows, kv_cols // heads), BF16),
                pltpu.VMEM((heads, q_rows, kv_cols // heads), BF16),
                pltpu.VMEM((4, q_rows // 4, width), BF16),
                pltpu.VMEM((2, q_rows // 4, width), BF16),
                pltpu.VMEM((q_rows // 4, width), BF16),
                pltpu.VMEM((q_rows // 4, width), BF16),
                dma((4,)),
                dma((n_ep,)), dma((n_ep,)),
                dma((3, n_ep)), dma((3, n_ep)),
                dma((n_ep,)), dma((n_ep,)),
                dma((3, 2)), dma((3, 2)),
                dma((n_ep,)), dma((n_ep,)),
                dma((2,)),dma((2,)),
                dma((4,)), dma((4,)),
                dma((4, half)), dma((4, half)), dma((4,)),
                dma((3,)), dma((3,)),
            ],
            compiler_params=pltpu.CompilerParams(
                collective_id=0, has_side_effects=True, vmem_limit_bytes=62 * 1024 * 1024
            ),
        )(
            head_lambda, queries, key_rows, value_rows, sub_gain.reshape(1, -1), expert_input,
            norm_gain.reshape(1, -1), route_ids.T, route_weight.T, out_weight,
            gate_weight[0], up_weight[0], down_weight[0],
        )
        return pl.pallas_call(
            settle,
            name="settle",
            out_shape=tuple(jax.ShapeDtypeStruct(o.shape, o.dtype) for o in outs),
            in_specs=[hbm] * 2,
            out_specs=(hbm, hbm),
            scratch_shapes=[pltpu.VMEM(o.shape, o.dtype) for o in outs] + [dma((2,)), dma((2,))],
        )(*outs)

    placed = (
        P("ep", "tp"), P("ep", "tp"), P("ep", "tp"), P("tp"), P(), P("tp", None), P("ep", None), P(),
        P("ep", None), P("ep", None), P("ep", None, "tp"), P("ep", None, "tp"), P("ep", "tp", None),
    )
    return jax.shard_map(
        shards, mesh=mesh, in_specs=placed,
        out_specs=(P(("ep", "tp"), None), P("ep", "tp")), check_vma=False,
    )
```

```python
import functools

import jax
import jax.numpy as jnp
from jax import lax
from jax.experimental import pallas as pl
from jax.experimental.pallas import tpu as pltpu
from jax.sharding import PartitionSpec as P

EPS = 1e-06
MESH = pl.DeviceIdType.MESH
F32 = jnp.float32
BF16 = jnp.bfloat16


def flip(index, bits):
    low = 1
    while low <= bits:
        if bits & low:
            index = index + low - 2 * low * ((index // low) % 2)
        low *= 2
    return index


def dot(a, b, dims=((1,), (0,)), precision=None):
    return lax.dot_general(a, b, (dims, ((), ())), precision=precision, preferred_element_type=F32)


def kernel(
    n_ep, cap, lam, q, k, v, gain, x, norm_gain, ids, route_w, wo_hbm, wg_hbm, wu_hbm, wd_hbm,
    mixer, expert,
    wo, wg, wu, wd, arr, hidden, part, sib, ysend, yrecv, res, ret, kbuf, vbuf,
    outb, nrm, info, nrm_in, info_in, spread, qx, qs, high, low, acc, top, mix, att, hp, hsib, hysend, hyrecv,
    w_sem, d_send, d_recv, f_send, f_recv, r_send, r_recv, s_send, s_recv, y_send, y_recv,
    g_send, g_recv, x_send, x_recv, kv_send, kv_recv, k2_send, h_send, h_recv,
):
    me = lax.axis_index("ep")
    tp = lax.axis_index("tp")
    half, quarter = n_ep // 2, n_ep // 4
    upper = me // half
    near = (upper * half, half)
    early = ((1 - upper) * half, quarter)
    late = ((1 - upper) * half + quarter, quarter)
    mate = flip(me, half + quarter)
    first = upper * half
    tokens, width = x.shape
    cols = width // 4
    units = wg.shape[1]
    sib_tp, y_tp = flip(tp, 1), flip(tp, 2)

    def remote(src, dst, ssem, rsem, where):
        return pltpu.make_async_remote_copy(
            src_ref=src, dst_ref=dst, send_sem=ssem, recv_sem=rsem,
            device_id=where, device_id_type=MESH,
        )

    weights = [
        pltpu.make_async_copy(a, b, w_sem.at[i])
        for i, (a, b) in enumerate(((wg_hbm, wg), (wu_hbm, wu), (wd_hbm, wd), (wo_hbm, wo)))
    ]
    for copy in weights:
        copy.start()

    barrier = pltpu.get_barrier_semaphore()
    for d in range(1, n_ep):
        pl.semaphore_signal(barrier, inc=1, device_id=(flip(me, d), tp), device_id_type=MESH)
    for d in range(1, 4):
        pl.semaphore_signal(barrier, inc=1, device_id=(me, flip(tp, d)), device_id_type=MESH)

    slots = n_ep * cap
    id0, id1 = ids[0:1, :], ids[1:2, :]
    index = lax.broadcasted_iota(jnp.int32, (max(n_ep, 8), tokens), 0)
    hot0, hot1 = (index == id0).astype(F32), (index == id1).astype(F32)
    earlier = (
        lax.broadcasted_iota(jnp.int32, (tokens, tokens), 0)
        < lax.broadcasted_iota(jnp.int32, (tokens, tokens), 1)
    ).astype(F32).astype(BF16)
    rank = dot((hot0 + hot1).astype(BF16), earlier)
    row0 = id0 * cap + (jnp.sum(rank * hot0, axis=0, keepdims=True) + 0.5).astype(jnp.int32)
    row1 = id1 * cap + (jnp.sum(rank * hot1, axis=0, keepdims=True) + 0.5).astype(jnp.int32)
    slot = lax.broadcasted_iota(jnp.int32, (slots, tokens), 0)
    here = lax.broadcasted_iota(jnp.int32, (half * cap, tokens), 0) + first * cap
    dispatch = ((here == row0) | (here == row1)).astype(F32).astype(BF16)
    wide = x[...].astype(F32)
    inv = lax.rsqrt(jnp.mean(wide * wide, axis=-1, keepdims=True) + EPS)
    mine = pl.ds(pl.multiple_of(tp * cols, cols), cols)
    normed = (x[:, mine].astype(F32) * inv * norm_gain[:, mine]).astype(BF16)
    nrm[...] = normed
    line = lax.broadcasted_iota(jnp.int32, (8, tokens), 0)
    info[...] = jnp.where(line == 0, row0, jnp.where(line == 1, row1, 0)).astype(F32)
    outb[...] = dot(dispatch, normed).astype(BF16).reshape(half, cap, cols)
    pl.semaphore_wait(barrier, n_ep - 1 + 3)

    def dispatch_to(at):
        return remote(outb.at[at - first], arr.at[tp, me], d_send.at[at], d_recv.at[me], (at, tp))

    def spread_to(at):
        return remote(
            spread.at[at - first], arr.at[tp, mate], d_send.at[flip(at, half)], d_recv.at[mate], (at, tp)
        )

    def dispatch_from(at):
        return remote(outb.at[0], arr.at[tp, at], d_send.at[at], d_recv.at[at], (at, tp))

    def to_mate(i):
        src, dst = ((info, info_in), (nrm, nrm_in))[i]
        return remote(src, dst, g_send.at[i], g_recv.at[i], (mate, tp))

    def sources(group):
        base, size = group
        return [flip(base + me % size, i) for i in range(size)]

    def others(group):
        return sources(group)[1:] if group is near else sources(group)

    def send(ds):
        for d in ds:
            dispatch_to(flip(me, d)).start()

    def send_mate():
        to_mate(0).start()
        to_mate(1).start()

    at_middle = (me // quarter == 1) | (me // quarter == 2)

    def expand(condition):
        @pl.when(condition)
        def _():
            to_mate(0).wait_recv()
            to_mate(1).wait_recv()
            place = here.astype(F32)
            pick = ((place == info_in[0:1]) | (place == info_in[1:2])).astype(F32).astype(BF16)
            spread[...] = dot(pick, nrm_in[...]).astype(BF16).reshape(half, cap, cols)
            for at in others(near):
                spread_to(at).start()
            arr[tp, mate] = spread[me - first]

    def own_rows():
        local = lax.broadcasted_iota(jnp.int32, (cap, tokens), 0) + me * cap
        pick = ((local == row0) | (local == row1)).astype(F32).astype(BF16)
        for t in range(4):
            at = slice(t * cols, (t + 1) * cols)
            rows = (x[:, at].astype(F32) * inv * norm_gain[:, at]).astype(BF16)
            arr[t, me] = dot(pick, rows).astype(BF16)

    def weigh():
        comb = jnp.where(slot == row0, route_w[0:1, :], 0.0) + jnp.where(
            slot == row1, route_w[1:2, :], 0.0
        )
        big = comb.astype(BF16).astype(F32)
        high[...] = comb.T.astype(BF16)
        low[...] = (comb - big).T.astype(BF16)

    def to_sib(src):
        return remote(
            arr.at[tp, src], arr.at[tp, src], f_send.at[0, src], f_recv.at[0, src], (me, sib_tp)
        )

    def to_y(src):
        return remote(
            arr.at[tp, src], arr.at[tp, src], f_send.at[1, src], f_recv.at[1, src], (me, y_tp)
        )

    def y_to_sib(src):
        return remote(
            arr.at[y_tp, src], arr.at[y_tp, src], f_send.at[2, src], f_recv.at[2, src], (me, sib_tp)
        )

    def forward(src):
        @pl.when(src != mate)
        def _():
            dispatch_from(src).wait_recv()

        to_y(src).start()
        to_sib(src).start()

    def forward_when(condition, srcs):
        @pl.when(condition)
        def _():
            for src in srcs:
                forward(src)

    def relay(src):
        to_y(src).wait_recv()
        y_to_sib(src).start()

    def arrived(src):
        to_sib(src).wait_recv()
        y_to_sib(src).wait_recv()

    def gate_up(group, lo, hi):
        base, rows = group[0], group[1] * cap
        got = [arr[t, pl.ds(base, group[1])].reshape(rows, cols) for t in range(4)]
        for lo in range(lo * 128, min(hi * 128, units), 256):
            n = min(256, units - lo)
            total = jnp.zeros((rows, 2 * n), F32)
            for t in range(4):
                at = slice(t * cols, (t + 1) * cols)
                w = jnp.concatenate([wg[at, lo:lo + n], wu[at, lo:lo + n]], axis=1)
                total += dot(got[t], w)
            g, u = total[:, :n], total[:, n:]
            hidden[:rows, lo:lo + n] = (g / (1.0 + jnp.exp(-g)) * u).astype(BF16)

    def down(group, r):
        base, rows = group[0], group[1] * cap
        at = pl.ds(pl.multiple_of(flip(tp, r) * cols, cols), cols)
        out = dot(hidden[:rows], wd[:, at])
        part[r, pl.ds(base, group[1])] = out.astype(BF16).reshape(group[1], cap, cols)

    pairs = {}

    def pair(group, number, y):
        at = pl.ds(*group)
        c = remote(
            part.at[2 * y + 1, at], sib.at[y, at], s_send.at[number, y], s_recv.at[number, y], (me, sib_tp)
        )
        c.start()
        pairs[number, y] = c

    def over_y(at):
        return remote(ysend.at[at], yrecv.at[at], y_send.at[at], y_recv.at[at], (me, y_tp))

    def y_sum(group, number):
        pairs[number, 1].wait_recv()
        at = pl.ds(*group)
        ysend[at] = (part[2, at].astype(F32) + sib[1, at].astype(F32)).astype(BF16)

    def y_go(srcs):
        for to in srcs:
            over_y(to).start()

    def return_to(at):
        return remote(res.at[at], ret.at[me], r_send.at[at], r_recv.at[me], (at, tp))

    def return_from(at):
        return remote(res.at[at], ret.at[at], r_send.at[at], r_recv.at[at], (at, tp))

    def give_back(to, own=False):
        over_y(to).wait_recv()
        out = (
            part[0, to].astype(F32) + sib[0, to].astype(F32) + yrecv[to].astype(F32)
        ).astype(BF16)
        if own:
            ret[to] = out
        else:
            res[to] = out
            return_to(to).start()

    def give_back_when(condition, srcs):
        @pl.when(condition)
        def _():
            for at in srcs:
                give_back(at)

    def y_go_ordered(a, b):
        @pl.when(upper == 1)
        def _():
            y_go(a + b)

        @pl.when(upper == 0)
        def _():
            y_go(b + a)

    across = flip(me, 1)
    level, side = me // 2, me % 2
    levels = n_ep // 2
    pinch = levels // 2 - 1

    q_rows = q.shape[0]
    heads = lam.shape[0]
    pair_width = q.shape[1] // heads
    head_width = pair_width // 2
    other = 1 - side
    my_head = pl.ds(pl.multiple_of(side * pair_width, pair_width), pair_width)
    its_head = pl.ds(pl.multiple_of(other * pair_width, pair_width), pair_width)

    def swap(i):
        src, dst = ((k, kbuf.at[level, side]), (v, vbuf.at[level, side]), (q, qx.at[side]))[i]
        return remote(src.at[:, its_head], dst, x_send.at[i], x_recv.at[i], (across, tp))

    def swap_start():
        for i in range(3):
            swap(i).start()
        kbuf[level, side] = k[:, my_head]
        vbuf[level, side] = v[:, my_head]
        qx[side] = q[:, my_head]

    def swap_wait():
        for i in range(3):
            swap(i).wait_recv()

    def kv_copy(b, lev):
        buf = kbuf if b < 2 else vbuf
        at = buf.at[lev, b % 2]
        return remote(at, at, kv_send.at[b, lev], kv_recv.at[b, lev], (lax.rem(me + 2, n_ep), tp))

    def kv_skip(b):
        buf = kbuf if b < 2 else vbuf
        at = buf.at[level, b % 2]
        return remote(at, at, k2_send.at[b], kv_recv.at[b, level], (lax.rem(me + 4, n_ep), tp))

    def kv_first():
        @pl.when(level < levels - 1)
        def _():
            for b in range(2):
                kv_copy(b, level).start()

        @pl.when(level == pinch - 1)
        def _():
            for b in range(4):
                kv_skip(b).start()

        @pl.when(level < levels - 1)
        def _():
            for b in range(2, 4):
                kv_copy(b, level).start()

    def kv_hop(step):
        for b in range(4):
            kv_copy(b, level - step).wait_recv()
            kv_copy(b, level - step).start()

    def hop_lower():
        for step in range(1, pinch + 1):
            @pl.when((level >= step) & ((level < pinch) | ((level == pinch) & (step > 1))))
            def _():
                kv_hop(step)

    def hop_upper(lo, hi):
        for step in range(lo, hi):
            @pl.when((level > pinch) & (level < levels - 1) & (level >= step))
            def _():
                kv_hop(step)

    def kv_last(step):
        @pl.when(((level == levels - 1) & (level >= step)) | ((level == pinch) & (step == 1)))
        def _():
            for b in range(4):
                kv_copy(b, level - step).wait_recv()

    def kv_finish():
        def step(lev, carry):
            for b in range(4):
                kv_copy(b, lev).wait_send()
            return carry

        @pl.when((level < levels - 1) & (level != pinch))
        def _():
            lax.fori_loop(0, level + 1, step, 0)

        @pl.when(level == pinch)
        def _():
            lax.fori_loop(0, level - 1, step, 0)
            step(level, 0)

        @pl.when(level == pinch - 1)
        def _():
            for b in range(4):
                kv_skip(b).wait_send()

    both = 2 * q_rows
    head_lane = lax.broadcasted_iota(jnp.int32, (both, pair_width), 1)

    def with_ones(vb):
        return jnp.concatenate([vb, jnp.ones(vb.shape, BF16)], axis=1)

    def attend_own():
        qh = qx[...].reshape(both, pair_width).astype(F32) * (head_width ** -0.5)
        kb = kbuf[level].reshape(both, pair_width)
        vb = with_ones(vbuf[level].reshape(both, pair_width))
        for m in range(2):
            first = head_lane < head_width
            qs[m] = jnp.where(first if m == 0 else ~first, qh, 0.0).astype(BF16)
            s = dot(qs[m], kb, ((1,), (1,)))
            ok = lax.broadcasted_iota(jnp.int32, s.shape, 0) >= lax.broadcasted_iota(jnp.int32, s.shape, 1)
            s = jnp.where(ok, s, -1e30)
            t = jnp.max(s, axis=1, keepdims=True)
            w = jnp.exp(s - t)
            top[m] = t
            acc[m] = dot(w.astype(BF16), vb)

    def attend(lev):
        kb = kbuf[lev].reshape(both, pair_width)
        vb = with_ones(vbuf[lev].reshape(both, pair_width))
        for m in range(2):
            s = dot(qs[m], kb, ((1,), (1,)))
            old = top[m]
            t = jnp.maximum(old, jnp.max(s, axis=1, keepdims=True))
            w = jnp.exp(s - t)
            top[m] = t
            acc[m] = acc[m] * jnp.exp(old - t) + dot(w.astype(BF16), vb)

    def attend_at(step):
        @pl.when(level >= step)
        def _():
            attend(level - step)

    top_level = level == levels - 1

    def att_swap():
        return remote(mix.at[other], att.at[side], x_send.at[3], x_recv.at[3], (across, tp))

    def normalise():
        a = acc[:, :, :pair_width] / acc[:, :, pair_width:]
        contrast = a[0] - lam[side] * a[1]
        norm = lax.rsqrt(jnp.mean(contrast * contrast, axis=-1, keepdims=True) + EPS)
        mix[...] = (contrast * norm * gain[...]).astype(BF16).reshape(2, q_rows, pair_width)
        att_swap().start()
        att[side] = mix[side]

    def normalise_when(condition):
        @pl.when(condition)
        def _():
            normalise()

    def h_pair(y):
        return remote(
            hp.at[flip(tp, 2 * y + 1)], hsib.at[y], h_send.at[y], h_recv.at[y], (me, sib_tp)
        )

    def h_over():
        return remote(hysend, hyrecv, h_send.at[2], h_recv.at[2], (me, y_tp))

    def project():
        att_swap().wait_recv()
        rows = jnp.concatenate([att[h] for h in range(heads)], axis=1)
        hp[...] = dot(rows, wo[...]).astype(BF16).reshape(4, q_rows // 4, width)
        h_pair(1).start()
        h_pair(0).start()

    def project_when(condition):
        @pl.when(condition)
        def _():
            project()

    def h_send_over_when(condition):
        @pl.when(condition)
        def _():
            h_send_over()

    def h_send_over():
        h_pair(1).wait_recv()
        hysend[...] = (hp[y_tp].astype(F32) + hsib[1].astype(F32)).astype(BF16)
        h_over().start()

    def drain():
        for src in others(near) + sources(early) + sources(late):
            to_sib(src).wait_send()
            to_y(src).wait_send()
            y_to_sib(src).wait_send()
            return_to(src).wait_send()
        for src in sources(near) + sources(early) + sources(late):
            over_y(src).wait_send()
        for at in others(near):
            dispatch_to(at).wait_send()
            spread_to(at).wait_send()
        for i in range(2):
            to_mate(i).wait_send()
        for c in pairs.values():
            c.wait_send()
        for y in range(2):
            h_pair(y).wait_send()
        for i in range(3):
            swap(i).wait_send()
        att_swap().wait_send()
        kv_finish()

    def mix_out():
        h_pair(0).wait_recv()
        h_over().wait()
        mixer[...] = (
            hp[tp].astype(F32) + hsib[0].astype(F32) + hyrecv[...].astype(F32)
        ).astype(BF16)

    def combine():
        for src in others(near) + sources(early) + sources(late):
            return_from(src).wait_recv()
        got = ret[...].reshape(slots, cols)
        expert[...] = (dot(high[...], got) + dot(low[...], got)).astype(BF16)

    send(range(1, half))
    send_mate()
    own_rows()
    weigh()
    swap_start()
    forward(others(near)[0])
    forward(others(near)[1])
    for at in others(near)[2:]: forward(at)
    expand(at_middle)
    relay(others(near)[0])
    swap_wait()
    expand(~at_middle)
    kv_first()
    for at in others(near)[1:]: relay(at)
    attend_own()
    for copy in weights[:2]: copy.wait()
    for at in others(near): arrived(at)
    gate_up(near, 0, 4)
    for at in sources(early): forward(at)
    gate_up(near, 4, 7)
    for at in sources(late)[:1]: forward(at)
    for at in sources(early)[:1]: relay(at)
    hop_upper(1, 2)
    weights[2].wait()
    for r in (3, 1): down(near, r)
    pair(near, 0, 1)
    pair(near, 0, 0)
    for at in sources(late)[1:]: forward(at)
    for at in sources(early)[1:]: relay(at)
    for r in (2, 0): down(near, r)
    y_sum(near, 0)
    y_go(sources(near)[:half // 2])
    for at in sources(early): arrived(at)
    gate_up(early, 0, 7)
    for at in sources(late)[:1]: relay(at)
    hop_lower()
    down(early, 3)
    pair(early, 1, 1)
    down(early, 2)
    for at in sources(late)[1:]: relay(at)
    down(early, 1)
    pair(early, 1, 0)
    down(early, 0)
    y_sum(early, 1)
    y_go(sources(early))
    for at in sources(late): arrived(at)
    gate_up(late, 0, 7)
    hop_upper(2, levels)
    down(late, 3)
    pair(late, 2, 1)
    down(late, 2)
    down(late, 1)
    pair(late, 2, 0)
    down(late, 0)
    y_sum(late, 2)
    y_go(sources(late) + sources(near)[half // 2:])
    pairs[0, 0].wait_recv()
    pairs[1, 0].wait_recv()
    for i, at in enumerate(sources(near)[:half // 2]): give_back(at, i == 0)
    for at in sources(early)[:quarter // 2]: give_back(at)
    kv_last(1)
    attend_at(1)
    for at in sources(early)[quarter // 2:]: give_back(at)
    for step in range(2, levels): kv_last(step); attend_at(step)
    normalise()
    weights[3].wait()
    project_when(upper == 0)
    pairs[2, 0].wait_recv()
    for at in sources(late): give_back(at)
    h_send_over_when(upper == 0)
    for at in sources(near)[half // 2:]: give_back(at)
    project_when(upper == 1)
    h_send_over_when(upper == 1)
    combine()
    drain()
    mix_out()


def settle(mixer_in, expert_in, mixer, expert, store):
    copies = [
        pltpu.make_async_copy(a, b, store.at[i])
        for i, (a, b) in enumerate(((mixer_in, mixer), (expert_in, expert)))
    ]
    for copy in copies:
        copy.start()
    for copy in copies:
        copy.wait()


def solution(mesh):
    n_ep = mesh.shape["ep"]

    def shards(
        queries, key_rows, value_rows, head_lambda, sub_gain, out_weight, expert_input, norm_gain,
        route_ids, route_weight, gate_weight, up_weight, down_weight,
    ):
        tokens, width = expert_input.shape
        cap = 5 * route_ids.shape[1] * tokens // (3 * n_ep)
        cap = -(-cap // 16) * 16
        cols = width // 4
        half = n_ep // 2
        units = gate_weight.shape[2]
        q_rows, kv_cols = queries.shape
        heads = head_lambda.shape[0]
        vm = pl.BlockSpec(memory_space=pltpu.VMEM)
        hbm = pl.BlockSpec(memory_space=pl.ANY)
        dma = pltpu.SemaphoreType.DMA
        outs = pl.pallas_call(
            functools.partial(kernel, n_ep, cap),
            name="both_halves",
            out_shape=(
                pltpu.VMEM((q_rows // 4, width), BF16),
                pltpu.VMEM((tokens, cols), BF16),
            ),
            in_specs=[pl.BlockSpec(memory_space=pltpu.SMEM)] + [vm] * 8 + [hbm] * 4,
            out_specs=(vm, vm),
            scratch_shapes=[
                pltpu.VMEM(out_weight.shape, BF16),
                pltpu.VMEM((width, units), BF16),
                pltpu.VMEM((width, units), BF16),
                pltpu.VMEM((units, width), BF16),
                pltpu.VMEM((4, n_ep, cap, cols), BF16),
                pltpu.VMEM((half * cap, units), BF16),
                pltpu.VMEM((4, n_ep, cap, cols), BF16),
                pltpu.VMEM((2, n_ep, cap, cols), BF16),
                pltpu.VMEM((n_ep, cap, cols), BF16),
                pltpu.VMEM((n_ep, cap, cols), BF16),
                pltpu.VMEM((n_ep, cap, cols), BF16),
                pltpu.VMEM((n_ep, cap, cols), BF16),
                pltpu.VMEM((half, 2, q_rows, kv_cols // heads), BF16),
                pltpu.VMEM((half, 2, q_rows, kv_cols // heads), BF16),
                pltpu.VMEM((half, cap, cols), BF16),
                pltpu.VMEM((tokens, cols), BF16),
                pltpu.VMEM((8, tokens), F32),
                pltpu.VMEM((tokens, cols), BF16),
                pltpu.VMEM((8, tokens), F32),
                pltpu.VMEM((half, cap, cols), BF16),
                pltpu.VMEM((2, q_rows, kv_cols // heads), BF16),
                pltpu.VMEM((2, 2 * q_rows, kv_cols // heads), BF16),
                pltpu.VMEM((tokens, n_ep * cap), BF16),
                pltpu.VMEM((tokens, n_ep * cap), BF16),
                pltpu.VMEM((2, 2 * q_rows, 2 * kv_cols // heads), F32),
                pltpu.VMEM((2, 2 * q_rows, 1), F32),
                pltpu.VMEM((2, q_rows, kv_cols // heads), BF16),
                pltpu.VMEM((heads, q_rows, kv_cols // heads), BF16),
                pltpu.VMEM((4, q_rows // 4, width), BF16),
                pltpu.VMEM((2, q_rows // 4, width), BF16),
                pltpu.VMEM((q_rows // 4, width), BF16),
                pltpu.VMEM((q_rows // 4, width), BF16),
                dma((4,)),
                dma((n_ep,)), dma((n_ep,)),
                dma((3, n_ep)), dma((3, n_ep)),
                dma((n_ep,)), dma((n_ep,)),
                dma((3, 2)), dma((3, 2)),
                dma((n_ep,)), dma((n_ep,)),
                dma((2,)),dma((2,)),
                dma((4,)), dma((4,)),
                dma((4, half)), dma((4, half)), dma((4,)),
                dma((3,)), dma((3,)),
            ],
            compiler_params=pltpu.CompilerParams(
                collective_id=0, has_side_effects=True, vmem_limit_bytes=62 * 1024 * 1024
            ),
        )(
            head_lambda, queries, key_rows, value_rows, sub_gain.reshape(1, -1), expert_input,
            norm_gain.reshape(1, -1), route_ids.T, route_weight.T, out_weight,
            gate_weight[0], up_weight[0], down_weight[0],
        )
        return pl.pallas_call(
            settle,
            name="settle",
            out_shape=tuple(jax.ShapeDtypeStruct(o.shape, o.dtype) for o in outs),
            in_specs=[vm] * 2,
            out_specs=(hbm, hbm),
            scratch_shapes=[dma((2,))],
        )(*[pltpu.with_memory_space_constraint(o, pltpu.VMEM) for o in outs])

    placed = (
        P("ep", "tp"), P("ep", "tp"), P("ep", "tp"), P("tp"), P(), P("tp", None), P("ep", None), P(),
        P("ep", None), P("ep", None), P("ep", None, "tp"), P("ep", None, "tp"), P("ep", "tp", None),
    )
    return jax.shard_map(
        shards, mesh=mesh, in_specs=placed,
        out_specs=(P(("ep", "tp"), None), P("ep", "tp")), check_vma=False,
    )
```

```python
import functools

import jax
import jax.numpy as jnp
from jax import lax
from jax.experimental import pallas as pl
from jax.experimental.pallas import tpu as pltpu
from jax.sharding import PartitionSpec as P

EPS = 1e-06
MESH = pl.DeviceIdType.MESH
F32 = jnp.float32
BF16 = jnp.bfloat16


def flip(index, bits):
    low = 1
    while low <= bits:
        if bits & low:
            index = index + low - 2 * low * ((index // low) % 2)
        low *= 2
    return index


def dot(a, b, dims=((1,), (0,)), precision=None):
    return lax.dot_general(a, b, (dims, ((), ())), precision=precision, preferred_element_type=F32)


def kernel(
    n_ep, cap, lam, q, k, v, gain, x, norm_gain, ids, route_w, wo_hbm, wg_hbm, wu_hbm, wd_hbm,
    mixer, expert,
    wo, wg, wu, wd, arr, hidden, part, sib, ysend, yrecv, res, ret, kbuf, vbuf,
    outb, nrm, info, nrm_in, info_in, spread, qx, qs, high, low, acc, top, mix, att, hp, hsib, hysend, hyrecv,
    w_sem, d_send, d_recv, f_send, f_recv, r_send, r_recv, s_send, s_recv, y_send, y_recv,
    g_send, g_recv, x_send, x_recv, kv_send, kv_recv, k2_send, h_send, h_recv,
):
    me = lax.axis_index("ep")
    tp = lax.axis_index("tp")
    half, quarter = n_ep // 2, n_ep // 4
    upper = me // half
    side_base = me // quarter * quarter
    near = (side_base, quarter)
    facing = (upper * n_ep + quarter - side_base, quarter)
    early = ((1 - upper) * half, quarter)
    late = ((1 - upper) * half + quarter, quarter)
    mate = flip(me, half + quarter)
    first = upper * half
    tokens, width = x.shape
    cols = width // 4
    units = wg.shape[1]
    sib_tp, y_tp = flip(tp, 1), flip(tp, 2)

    def remote(src, dst, ssem, rsem, where):
        return pltpu.make_async_remote_copy(
            src_ref=src, dst_ref=dst, send_sem=ssem, recv_sem=rsem,
            device_id=where, device_id_type=MESH,
        )

    weights = [
        pltpu.make_async_copy(a, b, w_sem.at[i])
        for i, (a, b) in enumerate(((wg_hbm, wg), (wu_hbm, wu), (wd_hbm, wd), (wo_hbm, wo)))
    ]
    for copy in weights:
        copy.start()

    barrier = pltpu.get_barrier_semaphore()
    for d in range(1, n_ep):
        pl.semaphore_signal(barrier, inc=1, device_id=(flip(me, d), tp), device_id_type=MESH)
    for d in range(1, 4):
        pl.semaphore_signal(barrier, inc=1, device_id=(me, flip(tp, d)), device_id_type=MESH)

    slots = n_ep * cap
    id0, id1 = ids[0:1, :], ids[1:2, :]
    index = lax.broadcasted_iota(jnp.int32, (max(n_ep, 8), tokens), 0)
    hot0, hot1 = (index == id0).astype(F32), (index == id1).astype(F32)
    earlier = (
        lax.broadcasted_iota(jnp.int32, (tokens, tokens), 0)
        < lax.broadcasted_iota(jnp.int32, (tokens, tokens), 1)
    ).astype(F32).astype(BF16)
    rank = dot((hot0 + hot1).astype(BF16), earlier)
    row0 = id0 * cap + (jnp.sum(rank * hot0, axis=0, keepdims=True) + 0.5).astype(jnp.int32)
    row1 = id1 * cap + (jnp.sum(rank * hot1, axis=0, keepdims=True) + 0.5).astype(jnp.int32)
    slot = lax.broadcasted_iota(jnp.int32, (slots, tokens), 0)
    here = lax.broadcasted_iota(jnp.int32, (half * cap, tokens), 0) + first * cap
    dispatch = ((here == row0) | (here == row1)).astype(F32).astype(BF16)
    wide = x[...].astype(F32)
    inv = lax.rsqrt(jnp.mean(wide * wide, axis=-1, keepdims=True) + EPS)
    mine = pl.ds(pl.multiple_of(tp * cols, cols), cols)
    normed = (x[:, mine].astype(F32) * inv * norm_gain[:, mine]).astype(BF16)
    nrm[...] = normed
    line = lax.broadcasted_iota(jnp.int32, (8, tokens), 0)
    info[...] = jnp.where(line == 0, row0, jnp.where(line == 1, row1, 0)).astype(F32)
    outb[...] = dot(dispatch, normed).astype(BF16).reshape(half, cap, cols)
    pl.semaphore_wait(barrier, n_ep - 1 + 3)

    def dispatch_to(at):
        return remote(outb.at[at - first], arr.at[tp, me], d_send.at[at], d_recv.at[me], (at, tp))

    def spread_to(at):
        return remote(
            spread.at[at - first], arr.at[tp, mate], d_send.at[flip(at, half)], d_recv.at[mate], (at, tp)
        )

    def dispatch_from(at):
        return remote(outb.at[0], arr.at[tp, at], d_send.at[at], d_recv.at[at], (at, tp))

    def to_mate(i):
        src, dst = ((info, info_in), (nrm, nrm_in))[i]
        return remote(src, dst, g_send.at[i], g_recv.at[i], (mate, tp))

    def sources(group):
        base, size = group
        return [flip(base + me % size, i) for i in range(size)]

    beside = sources(near)[1:]
    mates = beside + sources(facing)

    def send(ds):
        for d in ds:
            dispatch_to(flip(me, d)).start()

    def send_mate():
        to_mate(0).start()
        to_mate(1).start()

    at_middle = (me // quarter == 1) | (me // quarter == 2)

    def expand(condition):
        @pl.when(condition)
        def _():
            to_mate(0).wait_recv()
            to_mate(1).wait_recv()
            place = here.astype(F32)
            pick = ((place == info_in[0:1]) | (place == info_in[1:2])).astype(F32).astype(BF16)
            spread[...] = dot(pick, nrm_in[...]).astype(BF16).reshape(half, cap, cols)
            for at in mates:
                spread_to(at).start()
            arr[tp, mate] = spread[me - first]

    def own_rows():
        local = lax.broadcasted_iota(jnp.int32, (cap, tokens), 0) + me * cap
        pick = ((local == row0) | (local == row1)).astype(F32).astype(BF16)
        for t in range(4):
            at = slice(t * cols, (t + 1) * cols)
            rows = (x[:, at].astype(F32) * inv * norm_gain[:, at]).astype(BF16)
            arr[t, me] = dot(pick, rows).astype(BF16)

    def weigh():
        comb = jnp.where(slot == row0, route_w[0:1, :], 0.0) + jnp.where(
            slot == row1, route_w[1:2, :], 0.0
        )
        big = comb.astype(BF16).astype(F32)
        high[...] = comb.T.astype(BF16)
        low[...] = (comb - big).T.astype(BF16)

    def to_sib(src):
        return remote(
            arr.at[tp, src], arr.at[tp, src], f_send.at[0, src], f_recv.at[0, src], (me, sib_tp)
        )

    def to_y(src):
        return remote(
            arr.at[tp, src], arr.at[tp, src], f_send.at[1, src], f_recv.at[1, src], (me, y_tp)
        )

    def y_to_sib(src):
        return remote(
            arr.at[y_tp, src], arr.at[y_tp, src], f_send.at[2, src], f_recv.at[2, src], (me, sib_tp)
        )

    def forward(src):
        @pl.when(src != mate)
        def _():
            dispatch_from(src).wait_recv()

        to_y(src).start()
        to_sib(src).start()

    def forward_when(condition, srcs):
        @pl.when(condition)
        def _():
            for src in srcs:
                forward(src)

    def relay_when(condition, srcs):
        @pl.when(condition)
        def _():
            for src in srcs:
                relay(src)

    def relay(src):
        to_y(src).wait_recv()
        y_to_sib(src).start()

    def arrived(src):
        to_sib(src).wait_recv()
        y_to_sib(src).wait_recv()

    def gate_up(group, lo, hi):
        base, rows = group[0], group[1] * cap
        got = [arr[t, pl.ds(base, group[1])].reshape(rows, cols) for t in range(4)]
        for lo in range(lo * 128, min(hi * 128, units), 256):
            n = min(256, units - lo)
            total = jnp.zeros((rows, 2 * n), F32)
            for t in range(4):
                at = slice(t * cols, (t + 1) * cols)
                w = jnp.concatenate([wg[at, lo:lo + n], wu[at, lo:lo + n]], axis=1)
                total += dot(got[t], w)
            g, u = total[:, :n], total[:, n:]
            hidden[:rows, lo:lo + n] = (g / (1.0 + jnp.exp(-g)) * u).astype(BF16)

    def down(group, r):
        base, rows = group[0], group[1] * cap
        at = pl.ds(pl.multiple_of(flip(tp, r) * cols, cols), cols)
        out = dot(hidden[:rows], wd[:, at])
        part[r, pl.ds(base, group[1])] = out.astype(BF16).reshape(group[1], cap, cols)

    pairs = {}

    def pair(group, number, y):
        at = pl.ds(*group)
        c = remote(
            part.at[2 * y + 1, at], sib.at[y, at], s_send.at[number, y], s_recv.at[number, y], (me, sib_tp)
        )
        c.start()
        pairs[number, y] = c

    def over_y(at):
        return remote(ysend.at[at], yrecv.at[at], y_send.at[at], y_recv.at[at], (me, y_tp))

    def y_sum(group, number):
        pairs[number, 1].wait_recv()
        at = pl.ds(*group)
        ysend[at] = (part[2, at].astype(F32) + sib[1, at].astype(F32)).astype(BF16)

    def y_go(srcs):
        for to in srcs:
            over_y(to).start()

    def return_to(at):
        return remote(res.at[at], ret.at[me], r_send.at[at], r_recv.at[me], (at, tp))

    def return_from(at):
        return remote(res.at[at], ret.at[at], r_send.at[at], r_recv.at[at], (at, tp))

    def give_back(to, own=False):
        over_y(to).wait_recv()
        out = (
            part[0, to].astype(F32) + sib[0, to].astype(F32) + yrecv[to].astype(F32)
        ).astype(BF16)
        if own:
            ret[to] = out
        else:
            res[to] = out
            return_to(to).start()

    def give_back_when(condition, srcs):
        @pl.when(condition)
        def _():
            for at in srcs:
                give_back(at)

    def y_go_ordered(a, b):
        @pl.when(upper == 1)
        def _():
            y_go(a + b)

        @pl.when(upper == 0)
        def _():
            y_go(b + a)

    across = flip(me, 1)
    level, side = me // 2, me % 2
    levels = n_ep // 2
    pinch = levels // 2 - 1

    q_rows = q.shape[0]
    heads = lam.shape[0]
    pair_width = q.shape[1] // heads
    head_width = pair_width // 2
    other = 1 - side
    my_head = pl.ds(pl.multiple_of(side * pair_width, pair_width), pair_width)
    its_head = pl.ds(pl.multiple_of(other * pair_width, pair_width), pair_width)

    def swap(i):
        src, dst = ((k, kbuf.at[level, side]), (v, vbuf.at[level, side]), (q, qx.at[side]))[i]
        return remote(src.at[:, its_head], dst, x_send.at[i], x_recv.at[i], (across, tp))

    def swap_start():
        for i in range(3):
            swap(i).start()
        kbuf[level, side] = k[:, my_head]
        vbuf[level, side] = v[:, my_head]
        qx[side] = q[:, my_head]

    def swap_wait():
        for i in range(3):
            swap(i).wait_recv()

    def kv_copy(b, lev):
        buf = kbuf if b < 2 else vbuf
        at = buf.at[lev, b % 2]
        return remote(at, at, kv_send.at[b, lev], kv_recv.at[b, lev], (lax.rem(me + 2, n_ep), tp))

    def kv_skip(b):
        buf = kbuf if b < 2 else vbuf
        at = buf.at[level, b % 2]
        return remote(at, at, k2_send.at[b], kv_recv.at[b, level], (lax.rem(me + 4, n_ep), tp))

    def kv_first():
        @pl.when(level < levels - 1)
        def _():
            for b in range(4):
                kv_copy(b, level).start()

        @pl.when(level == pinch - 1)
        def _():
            for b in range(4):
                kv_skip(b).start()

    def kv_hop(step):
        for b in range(4):
            kv_copy(b, level - step).wait_recv()
            kv_copy(b, level - step).start()

    def hop_lower():
        for step in range(1, pinch + 1):
            @pl.when((level >= step) & ((level < pinch) | ((level == pinch) & (step > 1))))
            def _():
                kv_hop(step)

    def hop_upper(lo, hi):
        for step in range(lo, hi):
            @pl.when((level > pinch) & (level < levels - 1) & (level >= step))
            def _():
                kv_hop(step)

    def kv_last(step):
        @pl.when(((level == levels - 1) & (level >= step)) | ((level == pinch) & (step == 1)))
        def _():
            for b in range(4):
                kv_copy(b, level - step).wait_recv()

    def kv_finish():
        def step(lev, carry):
            for b in range(4):
                kv_copy(b, lev).wait_send()
            return carry

        @pl.when((level < levels - 1) & (level != pinch))
        def _():
            lax.fori_loop(0, level + 1, step, 0)

        @pl.when(level == pinch)
        def _():
            lax.fori_loop(0, level - 1, step, 0)
            step(level, 0)

        @pl.when(level == pinch - 1)
        def _():
            for b in range(4):
                kv_skip(b).wait_send()

    both = 2 * q_rows
    head_lane = lax.broadcasted_iota(jnp.int32, (both, pair_width), 1)

    def with_ones(vb):
        return jnp.concatenate([vb, jnp.ones(vb.shape, BF16)], axis=1)

    def attend_own():
        qh = qx[...].reshape(both, pair_width).astype(F32) * (head_width ** -0.5)
        kb = kbuf[level].reshape(both, pair_width)
        vb = with_ones(vbuf[level].reshape(both, pair_width))
        for m in range(2):
            first = head_lane < head_width
            qs[m] = jnp.where(first if m == 0 else ~first, qh, 0.0).astype(BF16)
            s = dot(qs[m], kb, ((1,), (1,)))
            ok = lax.broadcasted_iota(jnp.int32, s.shape, 0) >= lax.broadcasted_iota(jnp.int32, s.shape, 1)
            s = jnp.where(ok, s, -1e30)
            t = jnp.max(s, axis=1, keepdims=True)
            w = jnp.exp(s - t)
            top[m] = t
            acc[m] = dot(w.astype(BF16), vb)

    def attend(lev):
        kb = kbuf[lev].reshape(both, pair_width)
        vb = with_ones(vbuf[lev].reshape(both, pair_width))
        for m in range(2):
            s = dot(qs[m], kb, ((1,), (1,)))
            old = top[m]
            t = jnp.maximum(old, jnp.max(s, axis=1, keepdims=True))
            w = jnp.exp(s - t)
            top[m] = t
            acc[m] = acc[m] * jnp.exp(old - t) + dot(w.astype(BF16), vb)

    def attend_at(step):
        @pl.when(level >= step)
        def _():
            attend(level - step)

    top_level = level == levels - 1

    def attend_when(condition, step):
        @pl.when(condition & (level >= step))
        def _():
            attend(level - step)

    def att_swap():
        return remote(mix.at[other], att.at[side], x_send.at[3], x_recv.at[3], (across, tp))

    def normalise():
        a = acc[:, :, :pair_width] / acc[:, :, pair_width:]
        contrast = a[0] - lam[side] * a[1]
        norm = lax.rsqrt(jnp.mean(contrast * contrast, axis=-1, keepdims=True) + EPS)
        mix[...] = (contrast * norm * gain[...]).astype(BF16).reshape(2, q_rows, pair_width)
        att_swap().start()
        att[side] = mix[side]

    def normalise_when(condition):
        @pl.when(condition)
        def _():
            normalise()

    def h_pair(y):
        return remote(
            hp.at[flip(tp, 2 * y + 1)], hsib.at[y], h_send.at[y], h_recv.at[y], (me, sib_tp)
        )

    def h_over():
        return remote(hysend, hyrecv, h_send.at[2], h_recv.at[2], (me, y_tp))

    def project():
        att_swap().wait_recv()
        rows = jnp.concatenate([att[h] for h in range(heads)], axis=1)
        hp[...] = dot(rows, wo[...]).astype(BF16).reshape(4, q_rows // 4, width)
        h_pair(1).start()
        h_pair(0).start()

    def project_when(condition):
        @pl.when(condition)
        def _():
            project()

    def h_send_over_when(condition):
        @pl.when(condition)
        def _():
            h_send_over()

    def h_send_over():
        h_pair(1).wait_recv()
        hysend[...] = (hp[y_tp].astype(F32) + hsib[1].astype(F32)).astype(BF16)
        h_over().start()

    def drain():
        for src in mates + sources(early) + sources(late):
            to_sib(src).wait_send()
            to_y(src).wait_send()
            y_to_sib(src).wait_send()
            return_to(src).wait_send()
        for src in sources(near) + sources(facing) + sources(early) + sources(late):
            over_y(src).wait_send()
        for at in mates:
            dispatch_to(at).wait_send()
            spread_to(at).wait_send()
        for i in range(2):
            to_mate(i).wait_send()
        for c in pairs.values():
            c.wait_send()
        for y in range(2):
            h_pair(y).wait_send()
        for i in range(3):
            swap(i).wait_send()
        att_swap().wait_send()
        kv_finish()

    def mix_out():
        h_pair(0).wait_recv()
        h_over().wait()
        mixer[...] = (
            hp[tp].astype(F32) + hsib[0].astype(F32) + hyrecv[...].astype(F32)
        ).astype(BF16)

    def combine():
        for src in mates + sources(early) + sources(late):
            return_from(src).wait_recv()
        got = ret[...].reshape(slots, cols)
        expert[...] = (dot(high[...], got) + dot(low[...], got)).astype(BF16)

    send(range(1, quarter))
    send_mate()
    send(range(quarter, half))
    own_rows()
    weigh()
    swap_start()
    for at in beside: forward(at)
    expand(~at_middle)
    for at in beside: relay(at)
    expand(at_middle)
    swap_wait()
    kv_first()
    for at in sources(facing): forward(at)
    for copy in weights[:2]: copy.wait()
    for at in beside: arrived(at)
    gate_up(near, 0, 7)
    weights[2].wait()
    down(near, 3)
    pair(near, 0, 1)
    down(near, 1)
    pair(near, 0, 0)
    down(near, 2)
    down(near, 0)
    for at in sources(facing): relay(at)
    for at in sources(early): forward(at)
    for at in sources(late)[:quarter // 2]: forward(at)
    for at in sources(facing): arrived(at)
    gate_up(facing, 0, 7)
    for at in sources(late)[quarter // 2:]: forward(at)
    down(facing, 3)
    pair(facing, 3, 1)
    down(facing, 1)
    pair(facing, 3, 0)
    down(facing, 2)
    down(facing, 0)
    hop_upper(1, 2)
    for at in sources(early)[:quarter // 2]: relay(at)
    attend_own()
    for at in sources(early)[quarter // 2:]: relay(at)
    kv_last(1)
    attend_when(level <= 1, 1)
    normalise_when(level <= 1)
    y_sum(near, 0)
    y_go(sources(near))
    for at in sources(early): arrived(at)
    gate_up(early, 0, 7)
    for at in sources(late)[:quarter // 2]: relay(at)
    hop_lower()
    down(early, 3)
    pair(early, 1, 1)
    down(early, 2)
    for at in sources(late)[quarter // 2:]: relay(at)
    hop_upper(2, levels)
    down(early, 1)
    pair(early, 1, 0)
    down(early, 0)
    y_sum(early, 1)
    y_go(sources(early))
    for at in sources(late): arrived(at)
    gate_up(late, 0, 7)
    down(late, 3)
    pair(late, 2, 1)
    down(late, 2)
    down(late, 1)
    pair(late, 2, 0)
    down(late, 0)
    y_sum(late, 2)
    y_go(sources(late))
    y_sum(facing, 3)
    y_go(sources(facing))
    pairs[0, 0].wait_recv()
    pairs[1, 0].wait_recv()
    for i, at in enumerate(sources(near)): give_back(at, i == 0)
    weights[3].wait()
    for at in sources(early)[:quarter // 2]: give_back(at)
    project_when(level <= 1)
    attend_when(level > 1, 1)
    for at in sources(early)[quarter // 2:]: give_back(at)
    for step in range(2, levels): kv_last(step); attend_at(step)
    normalise_when(level > 1)
    h_send_over_when(level <= 1)
    pairs[2, 0].wait_recv()
    pairs[3, 0].wait_recv()
    for at in sources(late): give_back(at)
    project_when(level > 1)
    for at in sources(facing)[:quarter // 2]: give_back(at)
    h_send_over_when(level > 1)
    for at in sources(facing)[quarter // 2:]: give_back(at)
    combine()
    drain()
    mix_out()


def settle(mixer_in, expert_in, mixer, expert, store):
    copies = [
        pltpu.make_async_copy(a, b, store.at[i])
        for i, (a, b) in enumerate(((mixer_in, mixer), (expert_in, expert)))
    ]
    for copy in copies:
        copy.start()
    for copy in copies:
        copy.wait()


def solution(mesh):
    n_ep = mesh.shape["ep"]

    def shards(
        queries, key_rows, value_rows, head_lambda, sub_gain, out_weight, expert_input, norm_gain,
        route_ids, route_weight, gate_weight, up_weight, down_weight,
    ):
        tokens, width = expert_input.shape
        cap = 5 * route_ids.shape[1] * tokens // (3 * n_ep)
        cap = -(-cap // 16) * 16
        cols = width // 4
        half = n_ep // 2
        units = gate_weight.shape[2]
        q_rows, kv_cols = queries.shape
        heads = head_lambda.shape[0]
        vm = pl.BlockSpec(memory_space=pltpu.VMEM)
        hbm = pl.BlockSpec(memory_space=pl.ANY)
        dma = pltpu.SemaphoreType.DMA
        outs = pl.pallas_call(
            functools.partial(kernel, n_ep, cap),
            name="both_halves",
            out_shape=(
                pltpu.VMEM((q_rows // 4, width), BF16),
                pltpu.VMEM((tokens, cols), BF16),
            ),
            in_specs=[pl.BlockSpec(memory_space=pltpu.SMEM)] + [vm] * 8 + [hbm] * 4,
            out_specs=(vm, vm),
            scratch_shapes=[
                pltpu.VMEM(out_weight.shape, BF16),
                pltpu.VMEM((width, units), BF16),
                pltpu.VMEM((width, units), BF16),
                pltpu.VMEM((units, width), BF16),
                pltpu.VMEM((4, n_ep, cap, cols), BF16),
                pltpu.VMEM((half * cap, units), BF16),
                pltpu.VMEM((4, n_ep, cap, cols), BF16),
                pltpu.VMEM((2, n_ep, cap, cols), BF16),
                pltpu.VMEM((n_ep, cap, cols), BF16),
                pltpu.VMEM((n_ep, cap, cols), BF16),
                pltpu.VMEM((n_ep, cap, cols), BF16),
                pltpu.VMEM((n_ep, cap, cols), BF16),
                pltpu.VMEM((half, 2, q_rows, kv_cols // heads), BF16),
                pltpu.VMEM((half, 2, q_rows, kv_cols // heads), BF16),
                pltpu.VMEM((half, cap, cols), BF16),
                pltpu.VMEM((tokens, cols), BF16),
                pltpu.VMEM((8, tokens), F32),
                pltpu.VMEM((tokens, cols), BF16),
                pltpu.VMEM((8, tokens), F32),
                pltpu.VMEM((half, cap, cols), BF16),
                pltpu.VMEM((2, q_rows, kv_cols // heads), BF16),
                pltpu.VMEM((2, 2 * q_rows, kv_cols // heads), BF16),
                pltpu.VMEM((tokens, n_ep * cap), BF16),
                pltpu.VMEM((tokens, n_ep * cap), BF16),
                pltpu.VMEM((2, 2 * q_rows, 2 * kv_cols // heads), F32),
                pltpu.VMEM((2, 2 * q_rows, 1), F32),
                pltpu.VMEM((2, q_rows, kv_cols // heads), BF16),
                pltpu.VMEM((heads, q_rows, kv_cols // heads), BF16),
                pltpu.VMEM((4, q_rows // 4, width), BF16),
                pltpu.VMEM((2, q_rows // 4, width), BF16),
                pltpu.VMEM((q_rows // 4, width), BF16),
                pltpu.VMEM((q_rows // 4, width), BF16),
                dma((4,)),
                dma((n_ep,)), dma((n_ep,)),
                dma((3, n_ep)), dma((3, n_ep)),
                dma((n_ep,)), dma((n_ep,)),
                dma((4, 2)), dma((4, 2)),
                dma((n_ep,)), dma((n_ep,)),
                dma((2,)),dma((2,)),
                dma((4,)), dma((4,)),
                dma((4, half)), dma((4, half)), dma((4,)),
                dma((3,)), dma((3,)),
            ],
            compiler_params=pltpu.CompilerParams(
                collective_id=0, has_side_effects=True, vmem_limit_bytes=62 * 1024 * 1024
            ),
        )(
            head_lambda, queries, key_rows, value_rows, sub_gain.reshape(1, -1), expert_input,
            norm_gain.reshape(1, -1), route_ids.T, route_weight.T, out_weight,
            gate_weight[0], up_weight[0], down_weight[0],
        )
        return pl.pallas_call(
            settle,
            name="settle",
            out_shape=tuple(jax.ShapeDtypeStruct(o.shape, o.dtype) for o in outs),
            in_specs=[vm] * 2,
            out_specs=(hbm, hbm),
            scratch_shapes=[dma((2,))],
        )(*[pltpu.with_memory_space_constraint(o, pltpu.VMEM) for o in outs])

    placed = (
        P("ep", "tp"), P("ep", "tp"), P("ep", "tp"), P("tp"), P(), P("tp", None), P("ep", None), P(),
        P("ep", None), P("ep", None), P("ep", None, "tp"), P("ep", None, "tp"), P("ep", "tp", None),
    )
    return jax.shard_map(
        shards, mesh=mesh, in_specs=placed,
        out_specs=(P(("ep", "tp"), None), P("ep", "tp")), check_vma=False,
    )
```

```python
import functools

import jax
import jax.numpy as jnp
from jax import lax
from jax.experimental import pallas as pl
from jax.experimental.pallas import tpu as pltpu
from jax.sharding import PartitionSpec as P

EPS = 1e-06
MESH = pl.DeviceIdType.MESH
F32 = jnp.float32
BF16 = jnp.bfloat16


def flip(index, bits):
    low = 1
    while low <= bits:
        if bits & low:
            index = index + low - 2 * low * ((index // low) % 2)
        low *= 2
    return index


def dot(a, b, dims=((1,), (0,)), precision=None):
    return lax.dot_general(a, b, (dims, ((), ())), precision=precision, preferred_element_type=F32)


def kernel(
    n_ep, cap, lam, q, k, v, gain, x, norm_gain, ids, route_w, wo_hbm, wg_hbm, wu_hbm, wd_hbm,
    mixer, expert,
    wo, wg, wu, wd, arr, hidden, part, sib, ysend, yrecv, res, ret, kbuf, vbuf,
    outb, nrm, info, nrm_in, info_in, spread, qx, qs, high, low, acc, top, mix, att, hp, hsib, hysend, hyrecv,
    w_sem, d_send, d_recv, f_send, f_recv, r_send, r_recv, s_send, s_recv, y_send, y_recv,
    g_send, g_recv, x_send, x_recv, kv_send, kv_recv, k2_send, h_send, h_recv,
):
    me = lax.axis_index("ep")
    tp = lax.axis_index("tp")
    half, quarter = n_ep // 2, n_ep // 4
    upper = me // half
    side_base = me // quarter * quarter
    near = (side_base, quarter)
    facing = (upper * n_ep + quarter - side_base, quarter)
    early = ((1 - upper) * half, quarter)
    late = ((1 - upper) * half + quarter, quarter)
    mate = flip(me, half + quarter)
    first = upper * half
    tokens, width = x.shape
    cols = width // 4
    units = wg.shape[1]
    sib_tp, y_tp = flip(tp, 1), flip(tp, 2)

    def remote(src, dst, ssem, rsem, where):
        return pltpu.make_async_remote_copy(
            src_ref=src, dst_ref=dst, send_sem=ssem, recv_sem=rsem,
            device_id=where, device_id_type=MESH,
        )

    weights = [
        pltpu.make_async_copy(a, b, w_sem.at[i])
        for i, (a, b) in enumerate(((wg_hbm, wg), (wu_hbm, wu), (wd_hbm, wd), (wo_hbm, wo)))
    ]
    for copy in weights:
        copy.start()

    barrier = pltpu.get_barrier_semaphore()
    for d in range(1, n_ep):
        pl.semaphore_signal(barrier, inc=1, device_id=(flip(me, d), tp), device_id_type=MESH)
    for d in range(1, 4):
        pl.semaphore_signal(barrier, inc=1, device_id=(me, flip(tp, d)), device_id_type=MESH)

    slots = n_ep * cap
    id0, id1 = ids[0:1, :], ids[1:2, :]
    index = lax.broadcasted_iota(jnp.int32, (max(n_ep, 8), tokens), 0)
    hot0, hot1 = (index == id0).astype(F32), (index == id1).astype(F32)
    earlier = (
        lax.broadcasted_iota(jnp.int32, (tokens, tokens), 0)
        < lax.broadcasted_iota(jnp.int32, (tokens, tokens), 1)
    ).astype(F32).astype(BF16)
    rank = dot((hot0 + hot1).astype(BF16), earlier)
    row0 = id0 * cap + (jnp.sum(rank * hot0, axis=0, keepdims=True) + 0.5).astype(jnp.int32)
    row1 = id1 * cap + (jnp.sum(rank * hot1, axis=0, keepdims=True) + 0.5).astype(jnp.int32)
    slot = lax.broadcasted_iota(jnp.int32, (slots, tokens), 0)
    here = lax.broadcasted_iota(jnp.int32, (half * cap, tokens), 0) + first * cap
    dispatch = ((here == row0) | (here == row1)).astype(F32).astype(BF16)
    wide = x[...].astype(F32)
    inv = lax.rsqrt(jnp.mean(wide * wide, axis=-1, keepdims=True) + EPS)
    mine = pl.ds(pl.multiple_of(tp * cols, cols), cols)
    normed = (x[:, mine].astype(F32) * inv * norm_gain[:, mine]).astype(BF16)
    nrm[...] = normed
    line = lax.broadcasted_iota(jnp.int32, (8, tokens), 0)
    info[...] = jnp.where(line == 0, row0, jnp.where(line == 1, row1, 0)).astype(F32)
    outb[...] = dot(dispatch, normed).astype(BF16).reshape(half, cap, cols)
    pl.semaphore_wait(barrier, n_ep - 1 + 3)

    def dispatch_to(at):
        return remote(outb.at[at - first], arr.at[tp, me], d_send.at[at], d_recv.at[me], (at, tp))

    def spread_to(at):
        return remote(
            spread.at[at - first], arr.at[tp, mate], d_send.at[flip(at, half)], d_recv.at[mate], (at, tp)
        )

    def dispatch_from(at):
        return remote(outb.at[0], arr.at[tp, at], d_send.at[at], d_recv.at[at], (at, tp))

    def to_mate(i):
        src, dst = ((info, info_in), (nrm, nrm_in))[i]
        return remote(src, dst, g_send.at[i], g_recv.at[i], (mate, tp))

    def sources(group):
        base, size = group
        return [flip(base + me % size, i) for i in range(size)]

    beside = sources(near)[1:]
    mates = beside + sources(facing)

    def send(ds):
        for d in ds:
            dispatch_to(flip(me, d)).start()

    def send_mate():
        to_mate(0).start()
        to_mate(1).start()

    at_middle = (me // quarter == 1) | (me // quarter == 2)

    def expand(condition):
        @pl.when(condition)
        def _():
            to_mate(0).wait_recv()
            to_mate(1).wait_recv()
            place = here.astype(F32)
            pick = ((place == info_in[0:1]) | (place == info_in[1:2])).astype(F32).astype(BF16)
            spread[...] = dot(pick, nrm_in[...]).astype(BF16).reshape(half, cap, cols)
            for at in mates:
                spread_to(at).start()
            arr[tp, mate] = spread[me - first]

    def own_rows():
        local = lax.broadcasted_iota(jnp.int32, (cap, tokens), 0) + me * cap
        pick = ((local == row0) | (local == row1)).astype(F32).astype(BF16)
        for t in range(4):
            at = slice(t * cols, (t + 1) * cols)
            rows = (x[:, at].astype(F32) * inv * norm_gain[:, at]).astype(BF16)
            arr[t, me] = dot(pick, rows).astype(BF16)

    def weigh():
        comb = jnp.where(slot == row0, route_w[0:1, :], 0.0) + jnp.where(
            slot == row1, route_w[1:2, :], 0.0
        )
        big = comb.astype(BF16).astype(F32)
        high[...] = comb.T.astype(BF16)
        low[...] = (comb - big).T.astype(BF16)

    def to_sib(src):
        return remote(
            arr.at[tp, src], arr.at[tp, src], f_send.at[0, src], f_recv.at[0, src], (me, sib_tp)
        )

    def to_y(src):
        return remote(
            arr.at[tp, src], arr.at[tp, src], f_send.at[1, src], f_recv.at[1, src], (me, y_tp)
        )

    def y_to_sib(src):
        return remote(
            arr.at[y_tp, src], arr.at[y_tp, src], f_send.at[2, src], f_recv.at[2, src], (me, sib_tp)
        )

    def forward(src):
        @pl.when(src != mate)
        def _():
            dispatch_from(src).wait_recv()

        to_y(src).start()
        to_sib(src).start()

    def forward_when(condition, srcs):
        @pl.when(condition)
        def _():
            for src in srcs:
                forward(src)

    def relay_when(condition, srcs):
        @pl.when(condition)
        def _():
            for src in srcs:
                relay(src)

    def relay(src):
        to_y(src).wait_recv()
        y_to_sib(src).start()

    def arrived(src):
        to_sib(src).wait_recv()
        y_to_sib(src).wait_recv()

    def gate_up(group, lo, hi):
        base, rows = group[0], group[1] * cap
        got = [arr[t, pl.ds(base, group[1])].reshape(rows, cols) for t in range(4)]
        for lo in range(lo * 128, min(hi * 128, units), 256):
            n = min(256, units - lo)
            total = jnp.zeros((rows, 2 * n), F32)
            for t in range(4):
                at = slice(t * cols, (t + 1) * cols)
                w = jnp.concatenate([wg[at, lo:lo + n], wu[at, lo:lo + n]], axis=1)
                total += dot(got[t], w)
            g, u = total[:, :n], total[:, n:]
            hidden[:rows, lo:lo + n] = (g / (1.0 + jnp.exp(-g)) * u).astype(BF16)

    def down(group, r):
        base, rows = group[0], group[1] * cap
        at = pl.ds(pl.multiple_of(flip(tp, r) * cols, cols), cols)
        out = dot(hidden[:rows], wd[:, at])
        part[r, pl.ds(base, group[1])] = out.astype(BF16).reshape(group[1], cap, cols)

    pairs = {}

    def pair(group, number, y):
        at = pl.ds(*group)
        c = remote(
            part.at[2 * y + 1, at], sib.at[y, at], s_send.at[number, y], s_recv.at[number, y], (me, sib_tp)
        )
        c.start()
        pairs[number, y] = c

    def over_y(at):
        return remote(ysend.at[at], yrecv.at[at], y_send.at[at], y_recv.at[at], (me, y_tp))

    def y_sum(group, number):
        pairs[number, 1].wait_recv()
        at = pl.ds(*group)
        ysend[at] = (part[2, at].astype(F32) + sib[1, at].astype(F32)).astype(BF16)

    def y_go(srcs):
        for to in srcs:
            over_y(to).start()

    def return_to(at):
        return remote(res.at[at], ret.at[me], r_send.at[at], r_recv.at[me], (at, tp))

    def return_from(at):
        return remote(res.at[at], ret.at[at], r_send.at[at], r_recv.at[at], (at, tp))

    def give_back(to, own=False):
        over_y(to).wait_recv()
        out = (
            part[0, to].astype(F32) + sib[0, to].astype(F32) + yrecv[to].astype(F32)
        ).astype(BF16)
        if own:
            ret[to] = out
        else:
            res[to] = out
            return_to(to).start()

    def give_back_when(condition, srcs):
        @pl.when(condition)
        def _():
            for at in srcs:
                give_back(at)

    def y_go_ordered(a, b):
        @pl.when(upper == 1)
        def _():
            y_go(a + b)

        @pl.when(upper == 0)
        def _():
            y_go(b + a)

    across = flip(me, 1)
    level, side = me // 2, me % 2
    levels = n_ep // 2
    pinch = levels // 2 - 1

    q_rows = q.shape[0]
    heads = lam.shape[0]
    pair_width = q.shape[1] // heads
    head_width = pair_width // 2
    other = 1 - side
    my_head = pl.ds(pl.multiple_of(side * pair_width, pair_width), pair_width)
    its_head = pl.ds(pl.multiple_of(other * pair_width, pair_width), pair_width)

    def swap(i):
        src, dst = ((k, kbuf.at[level, side]), (v, vbuf.at[level, side]), (q, qx.at[side]))[i]
        return remote(src.at[:, its_head], dst, x_send.at[i], x_recv.at[i], (across, tp))

    def swap_start():
        for i in range(3):
            swap(i).start()
        kbuf[level, side] = k[:, my_head]
        vbuf[level, side] = v[:, my_head]
        qx[side] = q[:, my_head]

    def swap_wait():
        for i in range(3):
            swap(i).wait_recv()

    def kv_copy(b, lev):
        buf = vbuf if b else kbuf
        at = buf.at[lev]
        return remote(at, at, kv_send.at[b, lev], kv_recv.at[b, lev], (lax.rem(me + 2, n_ep), tp))

    def kv_skip(b):
        buf = vbuf if b else kbuf
        at = buf.at[level]
        return remote(at, at, k2_send.at[b], kv_recv.at[b, level], (lax.rem(me + 4, n_ep), tp))

    def kv_first():
        @pl.when(level < levels - 1)
        def _():
            for b in range(2):
                kv_copy(b, level).start()

        @pl.when(level == pinch - 1)
        def _():
            for b in range(2):
                kv_skip(b).start()

    def kv_hop(step):
        for b in range(2):
            kv_copy(b, level - step).wait_recv()
            kv_copy(b, level - step).start()

    def hop_lower():
        for step in range(1, pinch + 1):
            @pl.when((level >= step) & ((level < pinch) | ((level == pinch) & (step > 1))))
            def _():
                kv_hop(step)

    def hop_upper(lo, hi):
        for step in range(lo, hi):
            @pl.when((level > pinch) & (level < levels - 1) & (level >= step))
            def _():
                kv_hop(step)

    def kv_last(step):
        @pl.when(((level == levels - 1) & (level >= step)) | ((level == pinch) & (step == 1)))
        def _():
            for b in range(2):
                kv_copy(b, level - step).wait_recv()

    def kv_finish():
        def step(lev, carry):
            for b in range(2):
                kv_copy(b, lev).wait_send()
            return carry

        @pl.when((level < levels - 1) & (level != pinch))
        def _():
            lax.fori_loop(0, level + 1, step, 0)

        @pl.when(level == pinch)
        def _():
            lax.fori_loop(0, level - 1, step, 0)
            step(level, 0)

        @pl.when(level == pinch - 1)
        def _():
            for b in range(2):
                kv_skip(b).wait_send()

    both = 2 * q_rows
    head_lane = lax.broadcasted_iota(jnp.int32, (both, pair_width), 1)

    def with_ones(vb):
        return jnp.concatenate([vb, jnp.ones(vb.shape, BF16)], axis=1)

    def attend_own():
        qh = qx[...].reshape(both, pair_width).astype(F32) * (head_width ** -0.5)
        kb = kbuf[level].reshape(both, pair_width)
        vb = with_ones(vbuf[level].reshape(both, pair_width))
        for m in range(2):
            first = head_lane < head_width
            qs[m] = jnp.where(first if m == 0 else ~first, qh, 0.0).astype(BF16)
            s = dot(qs[m], kb, ((1,), (1,)))
            ok = lax.broadcasted_iota(jnp.int32, s.shape, 0) >= lax.broadcasted_iota(jnp.int32, s.shape, 1)
            s = jnp.where(ok, s, -1e30)
            t = jnp.max(s, axis=1, keepdims=True)
            w = jnp.exp(s - t)
            top[m] = t
            acc[m] = dot(w.astype(BF16), vb)

    def attend(lev):
        kb = kbuf[lev].reshape(both, pair_width)
        vb = with_ones(vbuf[lev].reshape(both, pair_width))
        for m in range(2):
            s = dot(qs[m], kb, ((1,), (1,)))
            old = top[m]
            t = jnp.maximum(old, jnp.max(s, axis=1, keepdims=True))
            w = jnp.exp(s - t)
            top[m] = t
            acc[m] = acc[m] * jnp.exp(old - t) + dot(w.astype(BF16), vb)

    def attend_at(step):
        @pl.when(level >= step)
        def _():
            attend(level - step)

    top_level = level == levels - 1

    def attend_when(condition, step):
        @pl.when(condition & (level >= step))
        def _():
            attend(level - step)

    def att_swap():
        return remote(mix.at[other], att.at[side], x_send.at[3], x_recv.at[3], (across, tp))

    def normalise():
        a = acc[:, :, :pair_width] / acc[:, :, pair_width:]
        contrast = a[0] - lam[side] * a[1]
        norm = lax.rsqrt(jnp.mean(contrast * contrast, axis=-1, keepdims=True) + EPS)
        mix[...] = (contrast * norm * gain[...]).astype(BF16).reshape(2, q_rows, pair_width)
        att_swap().start()
        att[side] = mix[side]

    def normalise_when(condition):
        @pl.when(condition)
        def _():
            normalise()

    def h_pair(y):
        return remote(
            hp.at[flip(tp, 2 * y + 1)], hsib.at[y], h_send.at[y], h_recv.at[y], (me, sib_tp)
        )

    def h_over():
        return remote(hysend, hyrecv, h_send.at[2], h_recv.at[2], (me, y_tp))

    def project():
        att_swap().wait_recv()
        rows = jnp.concatenate([att[h] for h in range(heads)], axis=1)
        hp[...] = dot(rows, wo[...]).astype(BF16).reshape(4, q_rows // 4, width)
        h_pair(1).start()
        h_pair(0).start()

    def project_when(condition):
        @pl.when(condition)
        def _():
            project()

    def h_send_over_when(condition):
        @pl.when(condition)
        def _():
            h_send_over()

    def h_send_over():
        h_pair(1).wait_recv()
        hysend[...] = (hp[y_tp].astype(F32) + hsib[1].astype(F32)).astype(BF16)
        h_over().start()

    def drain():
        for src in mates + sources(early) + sources(late):
            to_sib(src).wait_send()
            to_y(src).wait_send()
            y_to_sib(src).wait_send()
            return_to(src).wait_send()
        for src in sources(near) + sources(facing) + sources(early) + sources(late):
            over_y(src).wait_send()
        for at in mates:
            dispatch_to(at).wait_send()
            spread_to(at).wait_send()
        for i in range(2):
            to_mate(i).wait_send()
        for c in pairs.values():
            c.wait_send()
        for y in range(2):
            h_pair(y).wait_send()
        for i in range(3):
            swap(i).wait_send()
        att_swap().wait_send()
        kv_finish()

    def mix_out():
        h_pair(0).wait_recv()
        h_over().wait()
        mixer[...] = (
            hp[tp].astype(F32) + hsib[0].astype(F32) + hyrecv[...].astype(F32)
        ).astype(BF16)

    def combine():
        for src in mates + sources(early) + sources(late):
            return_from(src).wait_recv()
        got = ret[...].reshape(slots, cols)
        expert[...] = (dot(high[...], got) + dot(low[...], got)).astype(BF16)

    send(range(1, quarter))
    send_mate()
    send(range(quarter, half))
    own_rows()
    weigh()
    swap_start()
    for at in beside: forward(at)
    expand(~at_middle)
    for at in beside: relay(at)
    expand(at_middle)
    swap_wait()
    kv_first()
    for at in sources(facing): forward(at)
    for copy in weights[:2]: copy.wait()
    for at in beside: arrived(at)
    gate_up(near, 0, 7)
    weights[2].wait()
    down(near, 3)
    pair(near, 0, 1)
    down(near, 1)
    pair(near, 0, 0)
    down(near, 2)
    down(near, 0)
    for at in sources(facing): relay(at)
    for at in sources(early): forward(at)
    for at in sources(late)[:quarter // 2]: forward(at)
    for at in sources(facing): arrived(at)
    gate_up(facing, 0, 7)
    for at in sources(late)[quarter // 2:]: forward(at)
    down(facing, 3)
    pair(facing, 3, 1)
    down(facing, 1)
    pair(facing, 3, 0)
    down(facing, 2)
    down(facing, 0)
    hop_upper(1, 2)
    for at in sources(early)[:quarter // 2]: relay(at)
    attend_own()
    for at in sources(early)[quarter // 2:]: relay(at)
    kv_last(1)
    attend_when(level <= 1, 1)
    normalise_when(level <= 1)
    y_sum(near, 0)
    y_go(sources(near))
    for at in sources(early): arrived(at)
    gate_up(early, 0, 7)
    for at in sources(late)[:quarter // 2]: relay(at)
    hop_lower()
    down(early, 3)
    pair(early, 1, 1)
    down(early, 2)
    for at in sources(late)[quarter // 2:]: relay(at)
    hop_upper(2, levels)
    down(early, 1)
    pair(early, 1, 0)
    down(early, 0)
    y_sum(early, 1)
    y_go(sources(early))
    for at in sources(late): arrived(at)
    gate_up(late, 0, 7)
    down(late, 3)
    pair(late, 2, 1)
    down(late, 2)
    down(late, 1)
    pair(late, 2, 0)
    down(late, 0)
    y_sum(late, 2)
    y_go(sources(late))
    y_sum(facing, 3)
    y_go(sources(facing))
    pairs[0, 0].wait_recv()
    pairs[1, 0].wait_recv()
    for i, at in enumerate(sources(near)): give_back(at, i == 0)
    weights[3].wait()
    for at in sources(early)[:quarter // 2]: give_back(at)
    project_when(level <= 1)
    attend_when(level > 1, 1)
    for at in sources(early)[quarter // 2:]: give_back(at)
    for step in range(2, levels): kv_last(step); attend_at(step)
    normalise_when(level > 1)
    h_send_over_when(level <= 1)
    pairs[2, 0].wait_recv()
    pairs[3, 0].wait_recv()
    for at in sources(late): give_back(at)
    project_when(level > 1)
    for at in sources(facing)[:quarter // 2]: give_back(at)
    h_send_over_when(level > 1)
    for at in sources(facing)[quarter // 2:]: give_back(at)
    combine()
    drain()
    mix_out()


def settle(mixer_in, expert_in, mixer, expert, store):
    copies = [
        pltpu.make_async_copy(a, b, store.at[i])
        for i, (a, b) in enumerate(((mixer_in, mixer), (expert_in, expert)))
    ]
    for copy in copies:
        copy.start()
    for copy in copies:
        copy.wait()


def solution(mesh):
    n_ep = mesh.shape["ep"]

    def shards(
        queries, key_rows, value_rows, head_lambda, sub_gain, out_weight, expert_input, norm_gain,
        route_ids, route_weight, gate_weight, up_weight, down_weight,
    ):
        tokens, width = expert_input.shape
        cap = 5 * route_ids.shape[1] * tokens // (3 * n_ep)
        cap = -(-cap // 16) * 16
        cols = width // 4
        half = n_ep // 2
        units = gate_weight.shape[2]
        q_rows, kv_cols = queries.shape
        heads = head_lambda.shape[0]
        vm = pl.BlockSpec(memory_space=pltpu.VMEM)
        hbm = pl.BlockSpec(memory_space=pl.ANY)
        dma = pltpu.SemaphoreType.DMA
        outs = pl.pallas_call(
            functools.partial(kernel, n_ep, cap),
            name="both_halves",
            out_shape=(
                pltpu.VMEM((q_rows // 4, width), BF16),
                pltpu.VMEM((tokens, cols), BF16),
            ),
            in_specs=[pl.BlockSpec(memory_space=pltpu.SMEM)] + [vm] * 8 + [hbm] * 4,
            out_specs=(vm, vm),
            scratch_shapes=[
                pltpu.VMEM(out_weight.shape, BF16),
                pltpu.VMEM((width, units), BF16),
                pltpu.VMEM((width, units), BF16),
                pltpu.VMEM((units, width), BF16),
                pltpu.VMEM((4, n_ep, cap, cols), BF16),
                pltpu.VMEM((half * cap, units), BF16),
                pltpu.VMEM((4, n_ep, cap, cols), BF16),
                pltpu.VMEM((2, n_ep, cap, cols), BF16),
                pltpu.VMEM((n_ep, cap, cols), BF16),
                pltpu.VMEM((n_ep, cap, cols), BF16),
                pltpu.VMEM((n_ep, cap, cols), BF16),
                pltpu.VMEM((n_ep, cap, cols), BF16),
                pltpu.VMEM((half, 2, q_rows, kv_cols // heads), BF16),
                pltpu.VMEM((half, 2, q_rows, kv_cols // heads), BF16),
                pltpu.VMEM((half, cap, cols), BF16),
                pltpu.VMEM((tokens, cols), BF16),
                pltpu.VMEM((8, tokens), F32),
                pltpu.VMEM((tokens, cols), BF16),
                pltpu.VMEM((8, tokens), F32),
                pltpu.VMEM((half, cap, cols), BF16),
                pltpu.VMEM((2, q_rows, kv_cols // heads), BF16),
                pltpu.VMEM((2, 2 * q_rows, kv_cols // heads), BF16),
                pltpu.VMEM((tokens, n_ep * cap), BF16),
                pltpu.VMEM((tokens, n_ep * cap), BF16),
                pltpu.VMEM((2, 2 * q_rows, 2 * kv_cols // heads), F32),
                pltpu.VMEM((2, 2 * q_rows, 1), F32),
                pltpu.VMEM((2, q_rows, kv_cols // heads), BF16),
                pltpu.VMEM((heads, q_rows, kv_cols // heads), BF16),
                pltpu.VMEM((4, q_rows // 4, width), BF16),
                pltpu.VMEM((2, q_rows // 4, width), BF16),
                pltpu.VMEM((q_rows // 4, width), BF16),
                pltpu.VMEM((q_rows // 4, width), BF16),
                dma((4,)),
                dma((n_ep,)), dma((n_ep,)),
                dma((3, n_ep)), dma((3, n_ep)),
                dma((n_ep,)), dma((n_ep,)),
                dma((4, 2)), dma((4, 2)),
                dma((n_ep,)), dma((n_ep,)),
                dma((2,)),dma((2,)),
                dma((4,)), dma((4,)),
                dma((2, half)), dma((2, half)), dma((2,)),
                dma((3,)), dma((3,)),
            ],
            compiler_params=pltpu.CompilerParams(
                collective_id=0, has_side_effects=True, vmem_limit_bytes=62 * 1024 * 1024
            ),
        )(
            head_lambda, queries, key_rows, value_rows, sub_gain.reshape(1, -1), expert_input,
            norm_gain.reshape(1, -1), route_ids.T, route_weight.T, out_weight,
            gate_weight[0], up_weight[0], down_weight[0],
        )
        return pl.pallas_call(
            settle,
            name="settle",
            out_shape=tuple(jax.ShapeDtypeStruct(o.shape, o.dtype) for o in outs),
            in_specs=[vm] * 2,
            out_specs=(hbm, hbm),
            scratch_shapes=[dma((2,))],
        )(*[pltpu.with_memory_space_constraint(o, pltpu.VMEM) for o in outs])

    placed = (
        P("ep", "tp"), P("ep", "tp"), P("ep", "tp"), P("tp"), P(), P("tp", None), P("ep", None), P(),
        P("ep", None), P("ep", None), P("ep", None, "tp"), P("ep", None, "tp"), P("ep", "tp", None),
    )
    return jax.shard_map(
        shards, mesh=mesh, in_specs=placed,
        out_specs=(P(("ep", "tp"), None), P("ep", "tp")), check_vma=False,
    )
```
